128 devices in a mesh: ep: 16 (over z, x), tp: 8 (over y, core).
Axes of the slice: x: 4, y: 4, z: 4, core: 2. Of those that a mesh axis runs over, the one named last changes fastest.
Arguments:
- mixer_input: bfloat16 [16384, 2048], P(('ep', 'tp')), may hold values from -6 to 6
- log_decay: float32 [16384, 8], P('ep', 'tp'), may hold values from -0.8 to 0
- mixer_gain: float32 [2048], replicated, may hold values from 0.1 to 1.9
- query_weight: bfloat16 [2048, 1024], P(None, 'tp'), may hold values from -0.125 to 0.125
- key_weight: bfloat16 [2048, 1024], P(None, 'tp'), may hold values from -0.125 to 0.125
- value_weight: bfloat16 [2048, 2048], P(None, 'tp'), may hold values from -0.125 to 0.125
- gate_weight: bfloat16 [2048, 2048], P(None, 'tp'), may hold values from -0.125 to 0.125
- head_gain: float32 [2048], P('tp'), may hold values from 0.1 to 1.9
- output_weight: bfloat16 [2048, 2048], P('tp'), may hold values from -0.125 to 0.125
- expert_input: bfloat16 [16384, 2048], P(('ep', 'tp')), may hold values from -6 to 6
- expert_gain: float32 [2048], replicated, may hold values from 0.1 to 1.9
- routes: int32 [16384, 2], P(('ep', 'tp')), may hold values from 0 to 127, as said below
- group_weight: float32 [16384], P(('ep', 'tp')), may hold values from 0.3 to 1
- pair_weight: float32 [16384, 2], P(('ep', 'tp')), may hold values from 0.2 to 1
- expert_gate: bfloat16 [128, 2048, 1024], P(('ep', 'tp')), may hold values from -0.125 to 0.125
- expert_up: bfloat16 [128, 2048, 1024], P(('ep', 'tp')), may hold values from -0.125 to 0.125
- expert_down: bfloat16 [128, 1024, 2048], P(('ep', 'tp')), may hold values from -0.1875 to 0.1875
Outputs:
- mixer_output: bfloat16 [16384, 2048], P(('ep', 'tp'))
- expert_output: bfloat16 [16384, 2048], P(('ep', 'tp'))
The draws below stay inside these ranges and needn't reach their ends.
Inputs may be any that keep to these rules, and one draw needn't show every extreme that they name: `routes`: in the rows of one device each expert is named at most 3 times; one expert is named exactly 3 times in the rows of every device. A row names two different experts of the same group, a group being 32 consecutive expert numbers.
All inputs are finite; a program needn't handle non-finite values.
Results may differ from the reference program's by a relative error of at most 0.023.
Values may be sent and summed in bfloat16 or wider, within the bound.
No kernel may reach another device: no remote copies, remote signals or barrier semaphores. Data moves between devices by JAX's collectives and lax.ppermute only.
A program may use at most 128 MiB of HBM per device.

```python
import jax
import jax.numpy as jnp
from jax import lax

D = 2048
RETENTION_HEADS = 8
KEY_DIM = 128
VALUE_DIM = 256
SPAN = 512
FF = 1024
GROUPS = 4
TOPK = 2
TOK_B = 128
KEY_WIDTH = 1024
VALUE_WIDTH = 2048
SEG_ROWS = 1024
FIRST_POSITIONS = 16384
TOKENS_B = 16384
EXPERTS = 128
GROUP_SIZE = 32
CAP = 3
N_EP = 16
N_TP = 8


def draw_log_decay(key, part):
    split_random_keys = jax.random.split(jax.random.fold_in(key, 3), 7)
    fast_share = 0.5
    fast_heads = jax.random.uniform(split_random_keys[0], (RETENTION_HEADS,)) < fast_share
    fast_rate = 1.0 / jax.random.uniform(split_random_keys[1], (RETENTION_HEADS,), minval=30.0, maxval=100.0)
    slow_rate = jax.random.uniform(split_random_keys[2], (RETENTION_HEADS,), minval=0.1, maxval=0.5) / FIRST_POSITIONS
    head_rate = jnp.where(fast_heads, fast_rate, slow_rate)
    segments = FIRST_POSITIONS // SEG_ROWS
    segment_scale = jnp.exp(jax.random.uniform(split_random_keys[3], (segments,), minval=-0.7, maxval=0.7))
    row_scale = jnp.repeat(segment_scale, SEG_ROWS)
    jitter = jax.random.uniform(split_random_keys[4], (FIRST_POSITIONS, RETENTION_HEADS), minval=0.5, maxval=1.5)
    decay_factor = -head_rate[None, :] * row_scale[:, None] * jitter
    spike_rows = jax.random.randint(split_random_keys[5], (2,), 0, FIRST_POSITIONS)
    spike_loss = jnp.log(jax.random.uniform(split_random_keys[6], (2, RETENTION_HEADS), minval=0.5, maxval=0.8))
    position_list = jnp.arange(FIRST_POSITIONS)
    for index_value in range(2):
        decay_factor = decay_factor + jnp.where(position_list[:, None] == spike_rows[index_value], spike_loss[index_value][None, :], 0.0)
    return decay_factor.astype(jnp.float32)


def draw_routes(key, part):
    base_key = jax.random.fold_in(key, 7)
    chosen_key, block_base = jax.random.split(base_key)
    full_expert = jax.random.randint(chosen_key, (), 0, EXPERTS)
    pair_count = EXPERTS // 2

    def one_block(block_key):
        split_random_keys = jax.random.split(block_key, GROUPS + 3)
        orders = jnp.stack([jax.random.permutation(split_random_keys[group], GROUP_SIZE) for group in range(GROUPS)])
        labels = (orders + GROUP_SIZE * jnp.arange(GROUPS)[:, None]).reshape(-1).astype(jnp.int32)
        location = jnp.argmax(labels == full_expert)
        full_pair = location // 2
        slot_pairs = jnp.repeat(jnp.arange(pair_count), CAP)
        rank_order = jax.random.permutation(split_random_keys[GROUPS], pair_count * CAP)
        scores = jnp.where(slot_pairs == full_pair, rank_order, rank_order + pair_count * CAP)
        picked = jnp.argsort(scores)[:TOK_B]
        token_pairs = slot_pairs[picked][jax.random.permutation(split_random_keys[GROUPS + 1], TOK_B)]
        swapped = jax.random.randint(split_random_keys[GROUPS + 2], (TOK_B,), 0, 2)
        first_id = labels[2 * token_pairs + swapped]
        second = labels[2 * token_pairs + 1 - swapped]
        return jnp.stack([first_id, second], axis=1)
    block_keys = jax.random.split(block_base, TOKENS_B // TOK_B)
    return jax.vmap(one_block)(block_keys).reshape(TOKENS_B, TOPK).astype(jnp.int32)


def block_levels(key, extent, cuts, smallest, top_value):
    def one(dim, parts):
        draws = jax.random.uniform(jax.random.fold_in(jax.random.fold_in(key, 6), dim), (parts,), jnp.float32, smallest / len(cuts), top_value / len(cuts))
        return jnp.repeat(jnp.exp(draws), extent[dim] // parts).reshape((-1,) + (1,) * (len(extent) - dim - 1))

    loudness = one(*cuts[0])
    for cut in cuts[1:]:
        loudness = loudness * one(*cut)
    return loudness


def noise(key, shape, scale, reach, cuts=(), held_as=jnp.bfloat16):
    entries = jax.random.normal(key, shape, jnp.float32) * scale
    if len(cuts) > 0:
        entries = block_levels(key, shape, cuts, -0.22, 0.18) * entries
    return jnp.clip(entries, min=-reach, max=reach).astype(held_as)


def setup_inputs(seed: int = 0) -> dict:
    arg_keys = jax.random.split(jax.random.key(seed), 18)
    mixer_input = noise(arg_keys[0], (FIRST_POSITIONS, D), 1.0, 6.0, ((0, 128),))
    log_decay = draw_log_decay(jax.random.fold_in(arg_keys[17], 71), 0)
    mixer_gain = jnp.clip(1.0 + 0.18 * jax.random.normal(arg_keys[2], (D,), jnp.float32), 0.1, 1.9)
    query_weight = noise(arg_keys[3], (D, KEY_WIDTH), D ** -0.5, 0.125, ((1, 8),))
    key_weight = noise(arg_keys[4], (D, KEY_WIDTH), D ** -0.5, 0.125, ((1, 8),))
    value_weight = noise(arg_keys[5], (D, VALUE_WIDTH), D ** -0.5, 0.125, ((1, 8),))
    gate_weight = noise(arg_keys[6], (D, VALUE_WIDTH), D ** -0.5, 0.125, ((1, 8),))
    head_gain = jnp.clip(1.0 + 0.18 * jax.random.normal(arg_keys[7], (VALUE_WIDTH,), jnp.float32), 0.1, 1.9)
    output_weight = noise(arg_keys[8], (VALUE_WIDTH, D), VALUE_WIDTH ** -0.5, 0.125, ((0, 8),))
    expert_input = noise(arg_keys[9], (TOKENS_B, D), 1.0, 6.0, ((0, 128),))
    expert_gain = jnp.clip(1.0 + 0.18 * jax.random.normal(arg_keys[10], (D,), jnp.float32), 0.1, 1.9)
    routes = draw_routes(jax.random.fold_in(arg_keys[17], 71), 0)
    group_weight = jnp.clip(0.3 + 0.7 * jax.random.uniform(arg_keys[12], (TOKENS_B,), jnp.float32) ** block_levels(arg_keys[12], (TOKENS_B,), ((0, 128),), -0.2, 0.2), 0.3, 1.0)
    pair_weight = jnp.clip(0.2 + 0.8 * jax.random.uniform(arg_keys[13], (TOKENS_B, TOPK), jnp.float32) ** block_levels(arg_keys[13], (TOKENS_B, TOPK), ((0, 128),), -0.2, 0.2), 0.2, 1.0)
    expert_gate = noise(arg_keys[14], (EXPERTS, D, FF), D ** -0.5, 0.125, ((0, 128),))
    expert_up = noise(arg_keys[15], (EXPERTS, D, FF), D ** -0.5, 0.125, ((0, 128),))
    expert_down = noise(arg_keys[16], (EXPERTS, FF, D), FF ** -0.5, 0.1875, ((0, 128),))
    return dict(mixer_input=mixer_input, log_decay=log_decay, mixer_gain=mixer_gain, query_weight=query_weight, key_weight=key_weight, value_weight=value_weight, gate_weight=gate_weight, head_gain=head_gain, output_weight=output_weight, expert_input=expert_input, expert_gain=expert_gain, routes=routes, group_weight=group_weight, pair_weight=pair_weight, expert_gate=expert_gate, expert_up=expert_up, expert_down=expert_down)


EPSILON = 1e-05
THETA = 10000.0

def layer_norm(matrix, norm_gain):
    matrix = matrix.astype(jnp.float32)
    average = lax.optimization_barrier(jnp.mean(matrix, axis=-1, keepdims=True))
    centred = matrix - average
    spread = lax.optimization_barrier(jnp.mean(centred * centred, axis=-1, keepdims=True))
    return centred * lax.rsqrt(spread + EPSILON) * norm_gain.astype(jnp.float32)

def rotate(values, position):
    halfway = values.shape[-1] // 2
    frequency = THETA ** (-jnp.arange(halfway, dtype=jnp.float32) / halfway)
    angles = position[:, None] * frequency[None, :]
    cosine = jnp.cos(angles)[:, None, :]
    sine_part = jnp.sin(angles)[:, None, :]
    leading = values[..., :halfway]
    trailing = values[..., halfway:]
    return jnp.concatenate([leading * cosine - trailing * sine_part, trailing * cosine + leading * sine_part], axis=-1)

def block_step(state, inputs):
    query_rows, key_rows, value_rows, decay_factor = inputs
    span_len = query_rows.shape[0]
    cumulative = jnp.cumsum(decay_factor, axis=0)
    causal = jnp.arange(span_len)[:, None] >= jnp.arange(span_len)[None, :]
    log_gaps = cumulative.T[:, :, None] - cumulative.T[:, None, :]
    weight = jnp.where(causal[None], jnp.exp(jnp.minimum(log_gaps, 0.0)), 0.0)
    query_float = query_rows.astype(jnp.float32)
    key_float = key_rows.astype(jnp.float32)
    value_float = value_rows.astype(jnp.float32)
    scores = jnp.einsum('thd,shd->hts', query_float, key_float, precision=lax.Precision.HIGHEST)
    decayed = (scores * weight).astype(jnp.bfloat16).astype(jnp.float32)
    within = jnp.einsum('hts,she->the', decayed, value_float, precision=lax.Precision.HIGHEST)
    scaled = query_float * jnp.exp(cumulative)[:, :, None]
    carried = jnp.einsum('thd,hde->the', scaled, state, precision=lax.Precision.HIGHEST)
    span_total = cumulative[-1]
    remain = jnp.exp(span_total[None, :] - cumulative)
    update = jnp.einsum('shd,she->hde', key_float * remain[:, :, None], value_float, precision=lax.Precision.HIGHEST)
    return (state * jnp.exp(span_total)[:, None, None] + update, within + carried)

def token_mixer(mixer_input, log_decay, mixer_gain, query_weight, key_weight, value_weight, gate_weight, head_gain, output_weight):
    normed = layer_norm(mixer_input, mixer_gain).astype(jnp.bfloat16)

    def project(weight):
        return jnp.dot(normed, weight, preferred_element_type=jnp.float32).astype(jnp.bfloat16)
    query = project(query_weight).reshape(FIRST_POSITIONS, RETENTION_HEADS, KEY_DIM)
    keys_all = project(key_weight).reshape(FIRST_POSITIONS, RETENTION_HEADS, KEY_DIM)
    value = project(value_weight).reshape(FIRST_POSITIONS, RETENTION_HEADS, VALUE_DIM)
    gate = project(gate_weight).astype(jnp.float32)
    position = jnp.arange(FIRST_POSITIONS).astype(jnp.float32)
    rot_query = rotate(query.astype(jnp.float32), position).astype(jnp.bfloat16)
    rot_key = rotate(keys_all.astype(jnp.float32), position).astype(jnp.bfloat16)
    blocks = FIRST_POSITIONS // SPAN

    def split_blocks(tensor):
        return tensor.reshape((blocks, SPAN) + tensor.shape[1:])
    state_zero = jnp.zeros((RETENTION_HEADS, KEY_DIM, VALUE_DIM), jnp.float32)
    _, retained = lax.scan(block_step, state_zero, (split_blocks(rot_query), split_blocks(rot_key), split_blocks(value), split_blocks(log_decay)))
    retained = retained.reshape(FIRST_POSITIONS, RETENTION_HEADS, VALUE_DIM)
    average = lax.optimization_barrier(jnp.mean(retained, axis=-1, keepdims=True))
    centred = retained - average
    spread = lax.optimization_barrier(jnp.mean(centred * centred, axis=-1, keepdims=True))
    normed_heads = centred * lax.rsqrt(spread + EPSILON) * head_gain.reshape(RETENTION_HEADS, VALUE_DIM).astype(jnp.float32)
    gated = (jax.nn.silu(gate) * normed_heads.reshape(FIRST_POSITIONS, VALUE_WIDTH)).astype(jnp.bfloat16)
    group_cols = VALUE_WIDTH // N_TP
    summed = jnp.zeros((FIRST_POSITIONS, D), jnp.float32)
    for group in range(N_TP):
        lower = group * group_cols
        share_term = jnp.dot(gated[:, lower:lower + group_cols], output_weight[lower:lower + group_cols], preferred_element_type=jnp.float32).astype(jnp.bfloat16)
        summed = summed + share_term.astype(jnp.float32)
    return summed.astype(jnp.bfloat16)

def expert_mixture(expert_input, expert_gain, routes, group_weight, pair_weight, expert_gate, expert_up, expert_down):
    normed = layer_norm(expert_input, expert_gain).astype(jnp.bfloat16)
    flat_routes = routes.reshape(-1).astype(jnp.int32)
    capacity_rows = N_EP * N_TP * CAP
    mixing = (group_weight[:, None] * pair_weight).reshape(-1).astype(jnp.float32)

    def one_expert(carry, expert_id):
        matches = flat_routes == expert_id
        hits = jnp.nonzero(matches, size=capacity_rows, fill_value=0)[0].astype(jnp.int32)
        present = (jnp.arange(capacity_rows) < jnp.sum(matches)).astype(jnp.float32)
        token_ids = (hits // TOPK).astype(jnp.int32)
        gathered = normed[token_ids]
        gate_part = jnp.dot(gathered, expert_gate[expert_id], preferred_element_type=jnp.float32)
        up_part = jnp.dot(gathered, expert_up[expert_id], preferred_element_type=jnp.float32)
        hidden = (jax.nn.silu(gate_part) * up_part).astype(jnp.bfloat16)
        result = jnp.dot(hidden, expert_down[expert_id], preferred_element_type=jnp.float32).astype(jnp.bfloat16)
        contribution = result.astype(jnp.float32) * (mixing[hits] * present)[:, None]
        return (carry.at[token_ids].add(contribution), None)
    total, _ = lax.scan(one_expert, jnp.zeros((TOKENS_B, D), jnp.float32), jnp.arange(EXPERTS, dtype=jnp.int32))
    return total.astype(jnp.bfloat16)

def reference(mixer_input, log_decay, mixer_gain, query_weight, key_weight, value_weight, gate_weight, head_gain, output_weight, expert_input, expert_gain, routes, group_weight, pair_weight, expert_gate, expert_up, expert_down):
    mixer_output = token_mixer(mixer_input, log_decay, mixer_gain, query_weight, key_weight, value_weight, gate_weight, head_gain, output_weight)
    expert_output = expert_mixture(expert_input, expert_gain, routes, group_weight, pair_weight, expert_gate, expert_up, expert_down)
    return (mixer_output, expert_output)
```

```python
import functools

import jax
import jax.numpy as jnp
from jax import lax
from jax.experimental import pallas as pl
from jax.experimental.pallas import tpu as pltpu
from jax.sharding import PartitionSpec as P

KEY_DIM = 128
VALUE_DIM = 256
CHUNK = 256
CAP = 3
EPSILON = 1e-05
THETA = 10000.0
BF = jnp.bfloat16
F32 = jnp.float32
VM = pl.BlockSpec(memory_space=pltpu.VMEM)
SM = pl.BlockSpec(memory_space=pltpu.SMEM)


HBM = pl.BlockSpec(memory_space=pltpu.HBM)


def run(kernel, outs, args, scalars=0, flops=0, scratch=(), vmem=24 << 20, hbm=()):
    nbytes = sum(a.size * a.dtype.itemsize for a in args) + sum(
        o.size * o.dtype.itemsize for o in jax.tree.leaves(outs)
    )
    return pl.pallas_call(
        kernel,
        out_shape=outs,
        in_specs=[SM if i < scalars else HBM if i in hbm else VM for i in range(len(args))],
        out_specs=jax.tree.map(lambda _: VM, outs),
        scratch_shapes=list(scratch),
        compiler_params=pltpu.CompilerParams(vmem_limit_bytes=vmem),
        cost_estimate=pl.CostEstimate(flops=flops, bytes_accessed=nbytes, transcendentals=0),
    )(*args)


def after(value, *earlier):
    return lax.optimization_barrier((value, *earlier))[0]


def shape(dims, dtype=BF):
    return jax.ShapeDtypeStruct(dims, dtype)


def dot(a, b, ca=1, cb=0):
    return lax.dot_general(a, b, (((ca,), (cb,)), ((), ())), preferred_element_type=F32)


def silu(v):
    return v * (1.0 / (1.0 + jnp.exp(-v)))


def normalised(x, gain):
    x = x.astype(F32)
    centred = x - jnp.mean(x, axis=-1, keepdims=True)
    spread = jnp.mean(centred * centred, axis=-1, keepdims=True)
    return centred * lax.rsqrt(spread + EPSILON) * gain


def fetch(sems, *pairs):
    copies = [pltpu.make_async_copy(a, b, sems.at[i]) for i, (a, b) in enumerate(pairs)]
    for copy in copies:
        copy.start()
    for copy in copies:
        copy.wait()


def norm_kernel(x_hbm, gain_hbm, o_ref, x_ref, gain_ref, sems):
    fetch(sems, (x_hbm, x_ref), (gain_hbm, gain_ref))
    o_ref[...] = normalised(x_ref[...], gain_ref[...]).astype(BF)


def dispatch_kernel(x_hbm, gain_hbm, routes_hbm, o_ref, x_ref, gain_ref, routes_ref, sems):
    fetch(sems, (x_hbm, x_ref), (gain_hbm, gain_ref), (routes_hbm, routes_ref))
    rows = normalised(x_ref[...], gain_ref[...]).astype(BF)
    tokens = rows.shape[0]
    experts = o_ref.shape[0] * o_ref.shape[2]
    ids = lax.broadcasted_iota(jnp.int32, (experts, tokens), 0)
    named = (ids == routes_ref[0:1, :]) | (ids == routes_ref[1:2, :])
    named = jnp.where(named, 1.0, 0.0)
    before = lax.broadcasted_iota(jnp.int32, (tokens, tokens), 0) < lax.broadcasted_iota(
        jnp.int32, (tokens, tokens), 1
    )
    rank = dot(named.astype(BF), jnp.where(before, 1.0, 0.0).astype(BF))
    for slot in range(CAP):
        pick = jnp.where(rank == float(slot), named, 0.0).astype(BF)
        o_ref[:, slot] = dot(pick, rows).astype(BF).reshape(
            o_ref.shape[0], o_ref.shape[2], o_ref.shape[3]
        )


def permute_kernel(perm_ref, x_ref, o_ref):
    o_ref[...] = dot(perm_ref[...], x_ref[...]).astype(BF)


def expert_kernel(x_ref, gate_ref, up_ref, down_ref, perm_ref, o_ref, total):
    step = pl.program_id(0)
    x = x_ref[...]
    hidden = (silu(dot(x, gate_ref[...])) * dot(x, up_ref[...])).astype(BF)
    hidden = dot(perm_ref[...], hidden).astype(BF)
    part = dot(hidden, down_ref[...])

    @pl.when(step == 0)
    def _():
        total[...] = part

    @pl.when(step > 0)
    def _():
        total[...] += part

    @pl.when(step == pl.num_programs(0) - 1)
    def _():
        o_ref[...] = total[...].astype(BF)


def combine_kernel(rows_ref, routes_ref, group_ref, pair_ref, cols_ref, o_ref):
    tokens = routes_ref.shape[0]
    ids = cols_ref[0:1, :]
    slots = cols_ref[1:2, :].astype(F32)
    weight = group_ref[...] * pair_ref[...]
    first = routes_ref[:, 0:1] == ids
    second = routes_ref[:, 1:2] == ids
    named = jnp.where(first | second, 1.0, 0.0).astype(BF)
    before = lax.broadcasted_iota(jnp.int32, (tokens, tokens), 1) < lax.broadcasted_iota(
        jnp.int32, (tokens, tokens), 0
    )
    rank = dot(jnp.where(before, 1.0, 0.0).astype(BF), named)
    mix = jnp.where(first, weight[:, 0:1], 0.0) + jnp.where(second, weight[:, 1:2], 0.0)
    mix = jnp.where(rank == slots, mix, 0.0)
    high = mix.astype(BF)
    low = (mix - high.astype(F32)).astype(BF)
    rows = rows_ref[...]
    o_ref[...] = (dot(high, rows) + dot(low, rows)).astype(BF)


def project_kernel(*refs):
    *blocks, wq, wk, wv, wg, o_ref, w_ref, lhs, sems = refs
    copies, lower = [], 0
    for i, part in enumerate((wq, wk, wv, wg)):
        there = w_ref.at[:, lower : lower + part.shape[1]]
        copies.append(pltpu.make_async_copy(part, there, sems.at[i]))
        lower += part.shape[1]
    for copy in copies:
        copy.start()
    for i, block in enumerate(blocks):
        lhs[pl.ds(i * block.shape[0], block.shape[0]), :] = block[...]
    for copy in copies:
        copy.wait()
    o_ref[...] = dot(lhs[...], w_ref[...]).astype(BF)


def split_total(total, like):
    high = total.astype(BF).astype(F32)
    mid = (total - high).astype(BF).astype(F32)
    low = total - high - mid
    row = lax.broadcasted_iota(jnp.int32, like, 0)
    return jnp.where(row == 0, high, jnp.where(row == 1, mid, low)).astype(BF)


def assemble_kernel(
    src_ref, early_ref, b0_ref, b1_ref, w_ref, cos_ref, sin_ref, remain_ref, total_ref,
    q_ref, k_ref, v_ref, g_ref, state_ref, lhs, buf,
):
    rows = b0_ref.shape[0]
    lhs[0:rows, :] = b0_ref[...]
    lhs[rows : 2 * rows, :] = b1_ref[...]
    late = dot(lhs[...], w_ref[...]).astype(BF)
    early = early_ref.shape[0] // rows
    for i in range(early + 2):
        here = pl.ds(pl.multiple_of(src_ref[i] * rows, rows), rows)
        if i < early:
            buf[here, :] = early_ref[i * rows : (i + 1) * rows, :]
        else:
            buf[here, :] = late[(i - early) * rows : (i - early + 1) * rows, :]

    def rotated(lower):
        part = buf[:, lower : lower + KEY_DIM].astype(F32)
        swapped = pltpu.roll(part, KEY_DIM // 2, 1)
        return (part * cos_ref[...] + swapped * sin_ref[...]).astype(BF)

    q_ref[...] = rotated(0)
    key = rotated(KEY_DIM)
    k_ref[...] = key
    value = buf[:, 2 * KEY_DIM : 2 * KEY_DIM + VALUE_DIM]
    v_ref[...] = value
    g_ref[...] = buf[:, 2 * KEY_DIM + VALUE_DIM :]
    kept = (key.astype(F32) * remain_ref[...]).astype(BF)
    state_ref[0:KEY_DIM, :] = dot(kept, value, 0, 0).astype(BF)
    state_ref[KEY_DIM:, :] = split_total(total_ref[...], (8, VALUE_DIM))


def retention_kernel(q_ref, k_ref, v_ref, col_ref, row_ref, running_ref, o_ref, scaled_ref):
    state = None
    chunks = q_ref.shape[0] // CHUNK
    causal = lax.broadcasted_iota(jnp.int32, (CHUNK, CHUNK), 0) >= lax.broadcasted_iota(
        jnp.int32, (CHUNK, CHUNK), 1
    )
    for i in range(chunks):
        here = slice(i * CHUNK, (i + 1) * CHUNK)
        query, key, value = q_ref[here, :], k_ref[here, :], v_ref[here, :]
        col = col_ref[here, :]
        row = row_ref[i : i + 1, :]
        weight = jnp.where(causal, jnp.exp(jnp.minimum(col - row, 0.0)), 0.0)
        decayed = (dot(query, key, 1, 1) * weight).astype(BF)
        out = dot(decayed, value)
        wide = query.astype(F32)
        if state is not None:
            out = out + dot((wide * jnp.exp(col)).astype(BF), state.astype(BF))
        o_ref[here, :] = out
        scaled_ref[here, :] = (wide * jnp.exp(running_ref[here, :])).astype(BF)
        if i < chunks - 1:
            end = row[:, CHUNK - 1 : CHUNK]
            kept = (key.astype(F32) * jnp.exp(end - col)).astype(BF)
            update = dot(kept, value, 0, 0)
            state = update if state is None else state * jnp.exp(end) + update


def read_payload(ref):
    tail = ref[KEY_DIM:, :].astype(F32)
    return ref[0:KEY_DIM, :].astype(F32), tail[0:1] + tail[1:2] + tail[2:3]


def before_me(pos, parts):
    state, gone = 0.0, 0.0
    for j, (own, total) in enumerate(parts):
        between = 0.0
        for i, (_, other) in enumerate(parts):
            if i != j:
                inside = (pos[i] > pos[j]) & (pos[i] < pos[0])
                between = between + jnp.where(inside, other, 0.0)
        earlier = pos[j] < pos[0]
        state = state + jnp.where(earlier, own * jnp.exp(between), 0.0)
        gone = gone + jnp.where(earlier, total, 0.0)
    return state, gone


def x_kernel(pos_ref, p0, p1, p2, p3, prefix_ref, gone_ref, state_ref):
    pos = [pos_ref[i] for i in range(4)]
    parts = [read_payload(p) for p in (p0, p1, p2, p3)]
    state, gone = before_me(pos, parts)
    prefix_ref[...] = state
    gone_ref[...] = jnp.broadcast_to(jnp.exp(gone), gone_ref.shape)
    whole, total = 0.0, 0.0
    for j, (own, mine) in enumerate(parts):
        later = 0.0
        for i, (_, other) in enumerate(parts):
            if i != j:
                later = later + jnp.where(pos[i] > pos[j], other, 0.0)
        whole = whole + own * jnp.exp(later)
        total = total + mine
    state_ref[0:KEY_DIM, :] = whole.astype(BF)
    state_ref[KEY_DIM:, :] = split_total(total, (8, VALUE_DIM))


def gated_kernel(
    pos_ref, core_ref, p0, p1, p2, p3, prefix_ref, gone_ref, local_ref, scaled_ref, gate_ref,
    gain_ref, own_ref, twin_ref, buf,
):
    pos = [pos_ref[i] for i in range(4)]
    parts = [read_payload(p) for p in (p0, p1, p2, p3)]
    state, _ = before_me(pos, parts)
    incoming = (prefix_ref[...] + gone_ref[0:1, :] * state).astype(BF)
    retained = local_ref[...] + dot(scaled_ref[...], incoming)
    heads = normalised(retained, gain_ref[...])
    buf[...] = (silu(gate_ref[...].astype(F32)) * heads).astype(BF)
    core = core_ref[0]
    rows = own_ref.shape[0] // 4
    for y in range(4):
        there = slice(y * rows, (y + 1) * rows)
        own_ref[there, :] = buf[pl.ds(pl.multiple_of((2 * y + core) * rows, rows), rows), :]
        twin_ref[there, :] = buf[pl.ds(pl.multiple_of((2 * y + 1 - core) * rows, rows), rows), :]


def output_kernel(y_ref, own_ref, twin_ref, wo_ref, wt_ref, o0, o1, o2, o3, lhs, lht):
    rows = o0.shape[0]
    for k in range(4):
        here = slice(k * rows, (k + 1) * rows)
        there = pl.ds(pl.multiple_of(y_ref[k] * rows, rows), rows)
        lhs[here, :] = own_ref[there, :]
        lht[here, :] = twin_ref[there, :]
    out = (dot(lhs[...], wo_ref[...]) + dot(lht[...], wt_ref[...])).astype(BF)
    for k, ref in enumerate((o0, o1, o2, o3)):
        ref[...] = out[k * rows : (k + 1) * rows, :]


def sum_kernel(a, b, c, d, o_ref):
    o_ref[...] = (
        a[...].astype(F32) + b[...].astype(F32) + c[...].astype(F32) + d[...].astype(F32)
    ).astype(BF)


def core_swap(x):
    return lax.ppermute(x, "tp", [(t, t ^ 1) for t in range(8)])


def y_shift(x, k):
    return lax.ppermute(x, "tp", [(t, ((t // 2 + k) % 4) * 2 + t % 2) for t in range(8)])


def x_shift(x, k):
    return lax.ppermute(x, "ep", [(e, (e // 4) * 4 + (e + k) % 4) for e in range(16)])


def z_shift(x, k):
    return lax.ppermute(x, "ep", [(e, (e + 4 * k) % 16) for e in range(16)])


def exchange(x, axis):
    return lax.all_to_all(x, axis, split_axis=0, concat_axis=0, tiled=True)


def rotation(seg_rows):
    half = KEY_DIM // 2
    position = (lax.axis_index("ep") * seg_rows + jnp.arange(seg_rows, dtype=jnp.int32)).astype(F32)
    frequency = THETA ** (-jnp.arange(half, dtype=F32) / half)
    angles = position[:, None] * frequency[None, :]
    cosine, sine = jnp.cos(angles), jnp.sin(angles)
    return (
        jnp.concatenate([cosine, cosine], axis=1),
        jnp.concatenate([-sine, sine], axis=1),
    )


def local(
    mixer_input,
    log_decay,
    mixer_gain,
    query_weight,
    key_weight,
    value_weight,
    gate_weight,
    head_gain,
    output_weight,
    expert_input,
    expert_gain,
    routes,
    group_weight,
    pair_weight,
    expert_gate,
    expert_up,
    expert_down,
):
    rows, width = mixer_input.shape
    seg_rows = log_decay.shape[0]
    ep, tp = lax.axis_index("ep"), lax.axis_index("tp")
    y, core = tp // 2, tp % 2
    n_ep, n_tp = lax.axis_size("ep"), lax.axis_size("tp")
    slots = n_ep * n_tp * CAP

    sems = lambda n: pltpu.SemaphoreType.DMA((n,))
    normed = run(
        norm_kernel,
        shape((rows, width)),
        (mixer_input, mixer_gain[None]),
        hbm=(0, 1),
        scratch=(pltpu.VMEM((rows, width), BF), pltpu.VMEM((1, width), F32), sems(2)),
    )
    from_below, from_above = y_shift(normed, 1), y_shift(normed, -1)
    from_far = y_shift(normed, 2)
    twin = core_swap(normed)

    outgoing = run(
        dispatch_kernel,
        shape((n_ep, CAP, n_tp, width)),
        (after(expert_input, normed), expert_gain[None], routes.T),
        flops=2 * slots * rows * width,
        hbm=(0, 1, 2),
        scratch=(
            pltpu.VMEM((rows, width), BF),
            pltpu.VMEM((1, width), F32),
            pltpu.VMEM((2, rows), jnp.int32),
            sems(3),
        ),
    )
    staged = exchange(outgoing, "ep")

    twin_out = core_swap(output_weight)
    weights = (query_weight, key_weight, value_weight, gate_weight)
    cols = sum(w.shape[1] for w in weights)
    cosine, sine = rotation(seg_rows)
    per_chunk = log_decay.reshape(-1, CHUNK)
    chunk_sums = jnp.cumsum(per_chunk, axis=1)
    ends = jnp.cumsum(chunk_sums[:, -1])
    running = chunk_sums + (ends - chunk_sums[:, -1])[:, None]
    total = ends[-1:].reshape(1, 1)
    remain = jnp.exp(total - running).reshape(seg_rows, 1)

    below_twin, above_twin = core_swap(from_below), core_swap(from_above)
    early, joined = run(
        project_kernel,
        (shape((6 * rows, cols)), shape((width, cols))),
        (normed, twin, from_below, below_twin, from_above, above_twin, *weights),
        flops=2 * 6 * rows * width * cols,
        hbm=(6, 7, 8, 9),
        scratch=(pltpu.VMEM((6 * rows, width), BF), sems(4)),
    )
    far_twin = core_swap(from_far)
    away = jnp.array([0, 0, 3, 3, 1, 1, 2, 2], jnp.int32)
    flip = jnp.array([0, 1] * 4, jnp.int32)
    source = ((y + away) % 4) * 2 + (core + flip) % 2
    query, key, value, gate, state = run(
        assemble_kernel,
        (
            shape((seg_rows, KEY_DIM)),
            shape((seg_rows, KEY_DIM)),
            shape((seg_rows, VALUE_DIM)),
            shape((seg_rows, VALUE_DIM)),
            shape((KEY_DIM + 8, VALUE_DIM)),
        ),
        (source, early, from_far, far_twin, joined, cosine, sine, remain, total),
        scalars=1,
        flops=2 * 2 * rows * width * cols,
        scratch=(
            pltpu.VMEM((2 * rows, width), BF),
            pltpu.VMEM((seg_rows, cols), BF),
        ),
    )

    shifts = jnp.array([0, -1, 1, 2], jnp.int32)
    x_pos = (ep % 4 + shifts + 4) % 4
    z_pos = (ep // 4 + shifts + 4) % 4
    payloads = (state, x_shift(state, 1), x_shift(state, -1), x_shift(state, 2))
    local_out, scaled = run(
        retention_kernel,
        (shape((seg_rows, VALUE_DIM), F32), shape((seg_rows, KEY_DIM))),
        (query, key, value, chunk_sums.reshape(seg_rows, 1), chunk_sums, running.reshape(seg_rows, 1)),
        flops=8 * seg_rows * CHUNK * VALUE_DIM,
    )
    prefix, gone, plane = run(
        x_kernel,
        (
            shape((KEY_DIM, VALUE_DIM), F32),
            shape((8, VALUE_DIM), F32),
            shape((KEY_DIM + 8, VALUE_DIM)),
        ),
        (x_pos, *payloads),
        scalars=1,
    )
    planes = (plane, z_shift(plane, 1), z_shift(plane, -1), z_shift(plane, 2))
    own_gated, twin_gated = run(
        gated_kernel,
        (shape((4 * rows, VALUE_DIM)), shape((4 * rows, VALUE_DIM))),
        (z_pos, core.reshape(1), *planes, prefix, gone, local_out, scaled, gate, head_gain[None]),
        scalars=2,
        flops=2 * seg_rows * KEY_DIM * VALUE_DIM,
        scratch=(pltpu.VMEM((seg_rows, VALUE_DIM), BF),),
    )
    index = jnp.arange(slots, dtype=jnp.int32)
    deep = n_ep * CAP
    to_tp = ((index % deep) * n_tp + index // deep)[:, None] == index[None, :]
    to_ep = ((index % n_tp) * deep + index // n_tp)[:, None] == index[None, :]
    to_tp, to_ep = to_tp.astype(BF), to_ep.astype(BF)

    def turned(arrived):
        return run(
            permute_kernel,
            shape((slots, width)),
            (to_tp, arrived.reshape(slots, width)),
            flops=2 * slots * slots * width,
        ).reshape(n_tp, deep, width)

    staged = after(staged, state, to_tp, to_ep)
    tokens = exchange(after(turned(staged), from_far), "tp").reshape(slots, width)
    tokens = after(tokens, own_gated, twin_gated)
    hidden = expert_gate.shape[2]
    tile = 256
    results = pl.pallas_call(
        expert_kernel,
        grid=(hidden // tile,),
        out_shape=shape((slots, width)),
        in_specs=[
            pl.BlockSpec((slots, width), lambda f: (0, 0)),
            pl.BlockSpec((width, tile), lambda f: (0, f)),
            pl.BlockSpec((width, tile), lambda f: (0, f)),
            pl.BlockSpec((tile, width), lambda f: (f, 0)),
            pl.BlockSpec((slots, slots), lambda f: (0, 0)),
        ],
        out_specs=pl.BlockSpec((slots, width), lambda f: (0, 0)),
        scratch_shapes=[pltpu.VMEM((slots, width), F32)],
        compiler_params=pltpu.CompilerParams(
            vmem_limit_bytes=60 << 20, dimension_semantics=("arbitrary",)
        ),
        cost_estimate=pl.CostEstimate(
            flops=6 * slots * width * hidden, bytes_accessed=6 * width * hidden, transcendentals=0
        ),
    )(tokens, expert_gate[0], expert_up[0], expert_down[0], to_ep)
    other_gated = core_swap(twin_gated)
    y_order = (y + jnp.array([0, 1, 3, 2], jnp.int32)) % 4
    kept, up, down, far = run(
        output_kernel,
        tuple(shape((rows, width)) for _ in range(4)),
        (y_order, after(own_gated, results), other_gated, output_weight, twin_out),
        scalars=1,
        flops=2 * 4 * rows * 2 * VALUE_DIM * width,
        scratch=(pltpu.VMEM((4 * rows, VALUE_DIM), BF), pltpu.VMEM((4 * rows, VALUE_DIM), BF)),
    )
    got = (y_shift(up, 1), y_shift(down, -1), y_shift(far, 2))
    mixer_output = run(sum_kernel, shape((rows, width)), (kept, *got))

    returned = exchange(results.reshape(n_ep, CAP, n_tp, width), "ep")
    returned = after(returned, *got)
    returned = exchange(turned(returned), "tp").reshape(slots, width)
    column_expert = (index % deep) // CAP * n_tp + index // deep
    columns = jnp.stack([column_expert, index % CAP])
    expert_output = run(
        combine_kernel,
        shape((rows, width)),
        (returned, routes, group_weight[:, None], pair_weight, columns),
        flops=4 * slots * rows * width,
    )
    return (mixer_output, expert_output)


def solution(mesh):
    both = ("ep", "tp")
    return jax.shard_map(
        local,
        mesh=mesh,
        in_specs=(
            P(both, None),
            P("ep", "tp"),
            P(),
            P(None, "tp"),
            P(None, "tp"),
            P(None, "tp"),
            P(None, "tp"),
            P("tp"),
            P("tp", None),
            P(both, None),
            P(),
            P(both, None),
            P(both),
            P(both, None),
            P(both, None, None),
            P(both, None, None),
            P(both, None, None),
        ),
        out_specs=(P(both, None), P(both, None)),
        check_vma=False,
    )
```

```python
import jax
import jax.numpy as jnp
from jax import lax
from jax.experimental import pallas as pl
from jax.experimental.pallas import tpu as pltpu
from jax.sharding import PartitionSpec as P


KEY_DIM = 128
VALUE_DIM = 256
CHUNK = 256
CAP = 3
EPSILON = 1e-05
THETA = 10000.0
BF = jnp.bfloat16
F32 = jnp.float32
VM = pl.BlockSpec(memory_space=pltpu.VMEM)
SM = pl.BlockSpec(memory_space=pltpu.SMEM)


HBM = pl.BlockSpec(memory_space=pltpu.HBM)


def run(kernel, outs, args, scalars=0, flops=0, scratch=(), vmem=24 << 20, hbm=()):
    nbytes = sum(a.size * a.dtype.itemsize for a in args) + sum(
        o.size * o.dtype.itemsize for o in jax.tree.leaves(outs)
    )
    return pl.pallas_call(
        kernel,
        out_shape=outs,
        in_specs=[SM if i < scalars else HBM if i in hbm else VM for i in range(len(args))],
        out_specs=jax.tree.map(lambda _: VM, outs),
        scratch_shapes=list(scratch),
        compiler_params=pltpu.CompilerParams(vmem_limit_bytes=vmem),
        cost_estimate=pl.CostEstimate(flops=flops, bytes_accessed=nbytes, transcendentals=0),
    )(*args)


def after(value, *earlier):
    return lax.optimization_barrier((value, *earlier))[0]


def shape(dims, dtype=BF):
    return jax.ShapeDtypeStruct(dims, dtype)


def dot(a, b, ca=1, cb=0):
    return lax.dot_general(a, b, (((ca,), (cb,)), ((), ())), preferred_element_type=F32)


def silu(v):
    return v * (1.0 / (1.0 + jnp.exp(-v)))


def normalised(x, gain):
    x = x.astype(F32)
    centred = x - jnp.mean(x, axis=-1, keepdims=True)
    spread = jnp.mean(centred * centred, axis=-1, keepdims=True)
    return centred * lax.rsqrt(spread + EPSILON) * gain


def fetch(sems, *pairs):
    copies = [pltpu.make_async_copy(a, b, sems.at[i]) for i, (a, b) in enumerate(pairs)]
    for copy in copies:
        copy.start()
    for copy in copies:
        copy.wait()


def norm_kernel(x_hbm, gain_hbm, o_ref, x_ref, gain_ref, sems):
    fetch(sems, (x_hbm, x_ref), (gain_hbm, gain_ref))
    o_ref[...] = normalised(x_ref[...], gain_ref[...]).astype(BF)


def dispatch_kernel(x_hbm, gain_hbm, routes_hbm, o_ref, x_ref, gain_ref, routes_ref, sems):
    fetch(sems, (x_hbm, x_ref), (gain_hbm, gain_ref), (routes_hbm, routes_ref))
    rows = normalised(x_ref[...], gain_ref[...]).astype(BF)
    tokens = rows.shape[0]
    experts = o_ref.shape[0] * o_ref.shape[2]
    ids = lax.broadcasted_iota(jnp.int32, (experts, tokens), 0)
    named = (ids == routes_ref[0:1, :]) | (ids == routes_ref[1:2, :])
    named = jnp.where(named, 1.0, 0.0)
    before = lax.broadcasted_iota(jnp.int32, (tokens, tokens), 0) < lax.broadcasted_iota(
        jnp.int32, (tokens, tokens), 1
    )
    rank = dot(named.astype(BF), jnp.where(before, 1.0, 0.0).astype(BF))
    for slot in range(CAP):
        pick = jnp.where(rank == float(slot), named, 0.0).astype(BF)
        o_ref[:, slot] = dot(pick, rows).astype(BF).reshape(
            o_ref.shape[0], o_ref.shape[2], o_ref.shape[3]
        )


def permute_kernel(perm_ref, x_ref, o_ref):
    o_ref[...] = dot(perm_ref[...], x_ref[...]).astype(BF)


def hidden_kernel(x_ref, gate_ref, up_ref, perm_ref, o_ref):
    x = x_ref[...]
    hidden = (silu(dot(x, gate_ref[...])) * dot(x, up_ref[...])).astype(BF)
    o_ref[...] = dot(perm_ref[...], hidden).astype(BF)


def down_kernel(h_ref, down_ref, o_ref):
    o_ref[...] = dot(h_ref[...], down_ref[...]).reshape(o_ref.shape).astype(BF)


def combine_kernel(rows_ref, routes_ref, group_ref, pair_ref, cols_ref, o_ref):
    tokens = routes_ref.shape[0]
    ids = cols_ref[0:1, :]
    slots = cols_ref[1:2, :].astype(F32)
    weight = group_ref[...] * pair_ref[...]
    first = routes_ref[:, 0:1] == ids
    second = routes_ref[:, 1:2] == ids
    named = jnp.where(first | second, 1.0, 0.0).astype(BF)
    before = lax.broadcasted_iota(jnp.int32, (tokens, tokens), 1) < lax.broadcasted_iota(
        jnp.int32, (tokens, tokens), 0
    )
    rank = dot(jnp.where(before, 1.0, 0.0).astype(BF), named)
    mix = jnp.where(first, weight[:, 0:1], 0.0) + jnp.where(second, weight[:, 1:2], 0.0)
    mix = jnp.where(rank == slots, mix, 0.0)
    high = mix.astype(BF)
    low = (mix - high.astype(F32)).astype(BF)
    rows = rows_ref[...].reshape(ids.shape[1], rows_ref.shape[2])
    o_ref[...] = (dot(high, rows) + dot(low, rows)).astype(BF)


def project_kernel(*refs):
    *blocks, wq, wk, wv, wg, o_ref, w_ref, lhs, sems = refs
    copies, lower = [], 0
    for i, part in enumerate((wq, wk, wv, wg)):
        there = w_ref.at[:, lower : lower + part.shape[1]]
        copies.append(pltpu.make_async_copy(part, there, sems.at[i]))
        lower += part.shape[1]
    for copy in copies:
        copy.start()
    for i, block in enumerate(blocks):
        lhs[pl.ds(i * block.shape[0], block.shape[0]), :] = block[...]
    for copy in copies:
        copy.wait()
    o_ref[...] = dot(lhs[...], w_ref[...]).astype(BF)


def split_total(total, like):
    high = total.astype(BF).astype(F32)
    mid = (total - high).astype(BF).astype(F32)
    low = total - high - mid
    row = lax.broadcasted_iota(jnp.int32, like, 0)
    return jnp.where(row == 0, high, jnp.where(row == 1, mid, low)).astype(BF)


def prefix_sums(rows):
    n = rows.shape[1]
    upper = lax.broadcasted_iota(jnp.int32, (n, n), 0) <= lax.broadcasted_iota(jnp.int32, (n, n), 1)
    return lax.dot_general(
        rows, jnp.where(upper, 1.0, 0.0), (((1,), (0,)), ((), ())),
        precision=lax.Precision.HIGHEST, preferred_element_type=F32,
    )


def mixer_kernel(
    src_ref, early_ref, b0_ref, b1_ref, w_ref, turn_ref, decay_ref,
    g_ref, state_ref, local_ref, scaled_ref, lhs, buf,
):
    rows = b0_ref.shape[0]
    lhs[0:rows, :] = b0_ref[...]
    lhs[rows : 2 * rows, :] = b1_ref[...]
    late = dot(lhs[...], w_ref[...]).astype(BF)
    early = early_ref.shape[0] // rows
    for i in range(early + 2):
        here = pl.ds(pl.multiple_of(src_ref[i] * rows, rows), rows)
        if i < early:
            buf[here, :] = early_ref[i * rows : (i + 1) * rows, :]
        else:
            buf[here, :] = late[(i - early) * rows : (i - early + 1) * rows, :]
    g_ref[...] = buf[:, 2 * KEY_DIM + VALUE_DIM :]

    sums = prefix_sums(decay_ref[...])
    columns = sums.T
    causal = lax.broadcasted_iota(jnp.int32, (CHUNK, CHUNK), 0) >= lax.broadcasted_iota(
        jnp.int32, (CHUNK, CHUNK), 1
    )
    first = lax.broadcasted_iota(jnp.int32, (CHUNK, KEY_DIM), 1) < KEY_DIM // 2
    state, base = None, jnp.zeros((1, 1), F32)
    for i in range(buf.shape[0] // CHUNK):
        here = slice(i * CHUNK, (i + 1) * CHUNK)
        turn = turn_ref[here, :]
        other = pltpu.roll(turn, KEY_DIM // 2, 1)
        cosine = jnp.where(first, turn, other)
        sine = jnp.where(first, -other, turn)

        def rotated(lower):
            part = buf[here, lower : lower + KEY_DIM].astype(F32)
            return (part * cosine + pltpu.roll(part, KEY_DIM // 2, 1) * sine).astype(BF)

        query, key = rotated(0), rotated(KEY_DIM)
        value = buf[here, 2 * KEY_DIM : 2 * KEY_DIM + VALUE_DIM]
        row, col = sums[i : i + 1, :], columns[:, i : i + 1]
        weight = jnp.where(causal, jnp.exp(jnp.minimum(col - row, 0.0)), 0.0)
        decayed = (dot(query, key, 1, 1) * weight).astype(BF)
        out = dot(decayed, value)
        wide = query.astype(F32)
        if state is not None:
            out = out + dot((wide * jnp.exp(col)).astype(BF), state.astype(BF))
        local_ref[here, :] = out
        scaled_ref[here, :] = (wide * jnp.exp(col + base)).astype(BF)
        end = row[:, CHUNK - 1 : CHUNK]
        kept = (key.astype(F32) * jnp.exp(end - col)).astype(BF)
        update = dot(kept, value, 0, 0)
        state = update if state is None else state * jnp.exp(end) + update
        base = base + end
    state_ref[0:KEY_DIM, :] = state.astype(BF)
    state_ref[KEY_DIM:, :] = split_total(base, (8, VALUE_DIM))


def read_payload(ref):
    tail = ref[KEY_DIM:, :].astype(F32)
    return ref[0:KEY_DIM, :].astype(F32), tail[0:1] + tail[1:2] + tail[2:3]


def before_me(pos, parts):
    state, gone = 0.0, 0.0
    for j, (own, total) in enumerate(parts):
        between = 0.0
        for i, (_, other) in enumerate(parts):
            if i != j:
                inside = (pos[i] > pos[j]) & (pos[i] < pos[0])
                between = between + jnp.where(inside, other, 0.0)
        earlier = pos[j] < pos[0]
        state = state + jnp.where(earlier, own * jnp.exp(between), 0.0)
        gone = gone + jnp.where(earlier, total, 0.0)
    return state, gone


def x_kernel(pos_ref, p0, p1, p2, p3, prefix_ref, gone_ref, state_ref):
    pos = [pos_ref[i] for i in range(4)]
    parts = [read_payload(p) for p in (p0, p1, p2, p3)]
    state, gone = before_me(pos, parts)
    prefix_ref[...] = state
    gone_ref[...] = jnp.broadcast_to(jnp.exp(gone), gone_ref.shape)
    whole, total = 0.0, 0.0
    for j, (own, mine) in enumerate(parts):
        later = 0.0
        for i, (_, other) in enumerate(parts):
            if i != j:
                later = later + jnp.where(pos[i] > pos[j], other, 0.0)
        whole = whole + own * jnp.exp(later)
        total = total + mine
    state_ref[0:KEY_DIM, :] = whole.astype(BF)
    state_ref[KEY_DIM:, :] = split_total(total, (8, VALUE_DIM))


def gated_kernel(
    pos_ref, core_ref, p0, p1, p2, p3, prefix_ref, gone_ref, local_ref, scaled_ref, gate_ref,
    gain_ref, own_ref, twin_ref, buf,
):
    pos = [pos_ref[i] for i in range(4)]
    parts = [read_payload(p) for p in (p0, p1, p2, p3)]
    state, _ = before_me(pos, parts)
    incoming = (prefix_ref[...] + gone_ref[0:1, :] * state).astype(BF)
    retained = local_ref[...] + dot(scaled_ref[...], incoming)
    heads = normalised(retained, gain_ref[...])
    buf[...] = (silu(gate_ref[...].astype(F32)) * heads).astype(BF)
    core = core_ref[0]
    rows = own_ref.shape[0] // 4
    for y in range(4):
        there = slice(y * rows, (y + 1) * rows)
        own_ref[there, :] = buf[pl.ds(pl.multiple_of((2 * y + core) * rows, rows), rows), :]
        twin_ref[there, :] = buf[pl.ds(pl.multiple_of((2 * y + 1 - core) * rows, rows), rows), :]


def output_kernel(y_ref, own_ref, twin_ref, wo_ref, wt_ref, o0, o1, o2, o3, lhs, lht):
    rows = o0.shape[0]
    for k in range(4):
        here = slice(k * rows, (k + 1) * rows)
        there = pl.ds(pl.multiple_of(y_ref[k] * rows, rows), rows)
        lhs[here, :] = own_ref[there, :]
        lht[here, :] = twin_ref[there, :]
    out = (dot(lhs[...], wo_ref[...]) + dot(lht[...], wt_ref[...])).astype(BF)
    for k, ref in enumerate((o0, o1, o2, o3)):
        ref[...] = out[k * rows : (k + 1) * rows, :]


def sum_kernel(a, b, c, d, o_ref):
    o_ref[...] = (
        a[...].astype(F32) + b[...].astype(F32) + c[...].astype(F32) + d[...].astype(F32)
    ).astype(BF)


def core_swap(x):
    return lax.ppermute(x, "tp", [(t, t ^ 1) for t in range(8)])


def y_shift(x, k):
    return lax.ppermute(x, "tp", [(t, ((t // 2 + k) % 4) * 2 + t % 2) for t in range(8)])


def x_shift(x, k):
    return lax.ppermute(x, "ep", [(e, (e // 4) * 4 + (e + k) % 4) for e in range(16)])


def z_shift(x, k):
    return lax.ppermute(x, "ep", [(e, (e + 4 * k) % 16) for e in range(16)])


def exchange(x, axis):
    return lax.all_to_all(x, axis, split_axis=0, concat_axis=0, tiled=True)


def rotation(seg_rows):
    half = KEY_DIM // 2
    position = (lax.axis_index("ep") * seg_rows + jnp.arange(seg_rows, dtype=jnp.int32)).astype(F32)
    frequency = THETA ** (-jnp.arange(half, dtype=F32) / half)
    angles = position[:, None] * frequency[None, :]
    return jnp.concatenate([jnp.cos(angles), jnp.sin(angles)], axis=1)


def local(
    mixer_input,
    log_decay,
    mixer_gain,
    query_weight,
    key_weight,
    value_weight,
    gate_weight,
    head_gain,
    output_weight,
    expert_input,
    expert_gain,
    routes,
    group_weight,
    pair_weight,
    expert_gate,
    expert_up,
    expert_down,
):
    rows, width = mixer_input.shape
    seg_rows = log_decay.shape[0]
    ep, tp = lax.axis_index("ep"), lax.axis_index("tp")
    y, core = tp // 2, tp % 2
    n_ep, n_tp = lax.axis_size("ep"), lax.axis_size("tp")
    slots = n_ep * n_tp * CAP

    sems = lambda n: pltpu.SemaphoreType.DMA((n,))
    normed = run(
        norm_kernel,
        shape((rows, width)),
        (mixer_input, mixer_gain[None]),
        hbm=(0, 1),
        vmem=60 << 20,
        scratch=(pltpu.VMEM((rows, width), BF), pltpu.VMEM((1, width), F32), sems(2)),
    )
    from_below = y_shift(normed, 1)
    from_above = y_shift(normed, -1)
    from_far = y_shift(normed, 2)
    twin = core_swap(normed)

    outgoing = run(
        dispatch_kernel,
        shape((n_ep, CAP, n_tp, width)),
        (after(expert_input, normed), expert_gain[None], routes.T),
        flops=2 * slots * rows * width,
        hbm=(0, 1, 2),
        vmem=60 << 20,
        scratch=(
            pltpu.VMEM((rows, width), BF),
            pltpu.VMEM((1, width), F32),
            pltpu.VMEM((2, rows), jnp.int32),
            sems(3),
        ),
    )
    staged = exchange(outgoing, "ep")

    twin_out = core_swap(output_weight)
    weights = (query_weight, key_weight, value_weight, gate_weight)
    cols = sum(w.shape[1] for w in weights)
    turn = rotation(seg_rows)
    decay = jnp.pad(log_decay.reshape(-1, CHUNK), ((0, 8 - seg_rows // CHUNK), (0, 0)))

    below_twin, above_twin = core_swap(from_below), core_swap(from_above)
    early, joined = run(
        project_kernel,
        (shape((6 * rows, cols)), shape((width, cols))),
        (normed, twin, from_below, below_twin, from_above, above_twin, *weights),
        flops=2 * 6 * rows * width * cols,
        hbm=(6, 7, 8, 9),
        scratch=(pltpu.VMEM((6 * rows, width), BF), sems(4)),
    )
    far_twin = core_swap(from_far)
    away = jnp.array([0, 0, 3, 3, 1, 1, 2, 2], jnp.int32)
    flip = jnp.array([0, 1] * 4, jnp.int32)
    source = ((y + away) % 4) * 2 + (core + flip) % 2
    gate, state, local_out, scaled = run(
        mixer_kernel,
        (
            shape((seg_rows, VALUE_DIM)),
            shape((KEY_DIM + 8, VALUE_DIM)),
            shape((seg_rows, VALUE_DIM), F32),
            shape((seg_rows, KEY_DIM)),
        ),
        (source, early, from_far, far_twin, joined, turn, decay),
        scalars=1,
        flops=2 * 2 * rows * width * cols,
        scratch=(pltpu.VMEM((2 * rows, width), BF), pltpu.VMEM((seg_rows, cols), BF)),
    )

    index = jnp.arange(slots, dtype=jnp.int32)
    deep = n_ep * CAP
    to_tp = ((index % deep) * n_tp + index // deep)[:, None] == index[None, :]
    source_row = (index // CAP % n_tp) * deep + index // (CAP * n_tp) * CAP + index % CAP
    to_source = source_row[:, None] == index[None, :]
    to_tp, to_source = to_tp.astype(BF), to_source.astype(BF)
    turned = run(
        permute_kernel,
        shape((slots, width)),
        (to_tp, after(staged, state).reshape(slots, width)),
        flops=2 * slots * slots * width,
    )
    tokens = exchange(turned.reshape(n_tp, deep, width), "tp").reshape(slots, width)

    shifts = jnp.array([0, -1, 1, 2], jnp.int32)
    x_pos = (ep % 4 + shifts + 4) % 4
    z_pos = (ep // 4 + shifts + 4) % 4
    payloads = (state, x_shift(state, 1), x_shift(state, -1), x_shift(state, 2))
    prefix, gone, plane = run(
        x_kernel,
        (
            shape((KEY_DIM, VALUE_DIM), F32),
            shape((8, VALUE_DIM), F32),
            shape((KEY_DIM + 8, VALUE_DIM)),
        ),
        (x_pos, *payloads),
        scalars=1,
    )
    planes = (plane, z_shift(plane, 1), z_shift(plane, -1), z_shift(plane, 2))
    own_gated, twin_gated = run(
        gated_kernel,
        (shape((4 * rows, VALUE_DIM)), shape((4 * rows, VALUE_DIM))),
        (z_pos, core.reshape(1), *planes, prefix, gone, local_out, scaled, gate, head_gain[None]),
        scalars=2,
        flops=2 * seg_rows * KEY_DIM * VALUE_DIM,
        scratch=(pltpu.VMEM((seg_rows, VALUE_DIM), BF),),
    )
    inner = expert_gate.shape[2]
    tile, wide = 256, 512
    params = pltpu.CompilerParams(
        vmem_limit_bytes=60 << 20, dimension_semantics=("arbitrary",)
    )
    expand = pl.pallas_call(
        hidden_kernel,
        grid=(inner // tile,),
        out_shape=shape((slots, inner)),
        in_specs=[
            pl.BlockSpec((slots, width), lambda f: (0, 0)),
            pl.BlockSpec((width, tile), lambda f: (0, f)),
            pl.BlockSpec((width, tile), lambda f: (0, f)),
            pl.BlockSpec((slots, slots), lambda f: (0, 0)),
        ],
        out_specs=pl.BlockSpec((slots, tile), lambda f: (0, f)),
        compiler_params=params,
        cost_estimate=pl.CostEstimate(
            flops=4 * slots * width * inner, bytes_accessed=4 * width * inner, transcendentals=0
        ),
    )
    other_gated = core_swap(twin_gated)
    y_order = (y + jnp.array([0, 1, 3, 2], jnp.int32)) % 4
    kept, up, down, far = run(
        output_kernel,
        tuple(shape((rows, width)) for _ in range(4)),
        (y_order, own_gated, other_gated, output_weight, twin_out),
        scalars=1,
        flops=2 * 4 * rows * 2 * VALUE_DIM * width,
        scratch=(pltpu.VMEM((4 * rows, VALUE_DIM), BF), pltpu.VMEM((4 * rows, VALUE_DIM), BF)),
    )
    got_up = y_shift(up, 1)
    got_down = y_shift(down, -1)
    got_far = y_shift(far, 2)
    hidden = expand(after(tokens, kept), expert_gate[0], expert_up[0], to_source)
    mixer_output = run(sum_kernel, shape((rows, width)), (kept, got_up, got_down, got_far))

    project_down = pl.pallas_call(
        down_kernel,
        grid=(width // wide,),
        out_shape=shape((n_ep * n_tp, CAP, width)),
        in_specs=[
            pl.BlockSpec((slots, inner), lambda f: (0, 0)),
            pl.BlockSpec((inner, wide), lambda f: (0, f)),
        ],
        out_specs=pl.BlockSpec((n_ep * n_tp, CAP, wide), lambda f: (0, 0, f)),
        compiler_params=params,
        cost_estimate=pl.CostEstimate(
            flops=2 * slots * width * inner, bytes_accessed=2 * width * inner, transcendentals=0
        ),
    )
    results = project_down(hidden, expert_down[0])
    returned = exchange(results, ("ep", "tp"))
    columns = jnp.stack([index // CAP, index % CAP])
    expert_output = run(
        combine_kernel,
        shape((rows, width)),
        (returned, routes, group_weight[:, None], pair_weight, columns),
        flops=4 * slots * rows * width,
    )
    return (mixer_output, expert_output)


def solution(mesh):
    both = ("ep", "tp")
    return jax.shard_map(
        local,
        mesh=mesh,
        in_specs=(
            P(both, None),
            P("ep", "tp"),
            P(),
            P(None, "tp"),
            P(None, "tp"),
            P(None, "tp"),
            P(None, "tp"),
            P("tp"),
            P("tp", None),
            P(both, None),
            P(),
            P(both, None),
            P(both),
            P(both, None),
            P(both, None, None),
            P(both, None, None),
            P(both, None, None),
        ),
        out_specs=(P(both, None), P(both, None)),
        check_vma=False,
    )
```

```python
import functools

import jax
import jax.numpy as jnp
import numpy as np
from jax import lax
from jax.experimental import pallas as pl
from jax.experimental.pallas import tpu as pltpu
from jax.sharding import PartitionSpec as P


KEY_DIM = 128
VALUE_DIM = 256
CHUNK = 256
CAP = 3
EPSILON = 1e-05
THETA = 10000.0
BF = jnp.bfloat16
F32 = jnp.float32
VM = pl.BlockSpec(memory_space=pltpu.VMEM)
SM = pl.BlockSpec(memory_space=pltpu.SMEM)


HBM = pl.BlockSpec(memory_space=pltpu.HBM)


def run(kernel, outs, args, scalars=0, flops=0, scratch=(), vmem=24 << 20, hbm=(), hbm_outs=()):
    nbytes = sum(a.size * a.dtype.itemsize for a in args) + sum(
        o.size * o.dtype.itemsize for o in jax.tree.leaves(outs)
    )
    return pl.pallas_call(
        kernel,
        out_shape=outs,
        in_specs=[SM if i < scalars else HBM if i in hbm else VM for i in range(len(args))],
        out_specs=tuple(HBM if i in hbm_outs else VM for i in range(len(outs)))
        if isinstance(outs, tuple)
        else VM,
        scratch_shapes=list(scratch),
        compiler_params=pltpu.CompilerParams(vmem_limit_bytes=vmem),
        cost_estimate=pl.CostEstimate(flops=flops, bytes_accessed=nbytes, transcendentals=0),
    )(*args)


def after(value, *earlier):
    return lax.optimization_barrier((value, *earlier))[0]


def shape(dims, dtype=BF):
    return jax.ShapeDtypeStruct(dims, dtype)


def dot(a, b, ca=1, cb=0):
    return lax.dot_general(a, b, (((ca,), (cb,)), ((), ())), preferred_element_type=F32)


def silu(v):
    return v * (1.0 / (1.0 + jnp.exp(-v)))


def normalised(x, gain):
    x = x.astype(F32)
    centred = x - jnp.mean(x, axis=-1, keepdims=True)
    spread = jnp.mean(centred * centred, axis=-1, keepdims=True)
    return centred * lax.rsqrt(spread + EPSILON) * gain


def begin(sems, *pairs):
    copies = [pltpu.make_async_copy(a, b, sems.at[i]) for i, (a, b) in enumerate(pairs)]
    for copy in copies:
        copy.start()
    return copies


def finish(copies):
    for copy in copies:
        copy.wait()


def fetch(sems, *pairs):
    finish(begin(sems, *pairs))


def rows_of(ref, parts):
    pairs, lower = [], 0
    for part in parts:
        pairs.append((part, ref.at[lower : lower + part.shape[0], :]))
        lower += part.shape[0]
    return pairs


def norm_kernel(x_hbm, gain_hbm, o_ref, x_ref, gain_ref, sems):
    fetch(sems, (x_hbm, x_ref), (gain_hbm, gain_ref))
    o_ref[...] = normalised(x_ref[...], gain_ref[...]).astype(BF)


def dispatch_kernel(x_hbm, gain_hbm, routes_hbm, o_ref, x_ref, gain_ref, routes_ref, sems):
    fetch(sems, (x_hbm, x_ref), (gain_hbm, gain_ref), (routes_hbm, routes_ref))
    rows = normalised(x_ref[...], gain_ref[...]).astype(BF)
    tokens = rows.shape[0]
    experts = o_ref.shape[0] * o_ref.shape[2]
    ids = lax.broadcasted_iota(jnp.int32, (experts, tokens), 0)
    named = (ids == routes_ref[0:1, :]) | (ids == routes_ref[1:2, :])
    named = jnp.where(named, 1.0, 0.0)
    before = lax.broadcasted_iota(jnp.int32, (tokens, tokens), 0) < lax.broadcasted_iota(
        jnp.int32, (tokens, tokens), 1
    )
    rank = dot(named.astype(BF), jnp.where(before, 1.0, 0.0).astype(BF))
    for slot in range(CAP):
        pick = jnp.where(rank == float(slot), named, 0.0).astype(BF)
        o_ref[:, slot] = dot(pick, rows).astype(BF).reshape(
            o_ref.shape[0], o_ref.shape[2], o_ref.shape[3]
        )


def turn_kernel(index_ref, x_ref, o_ref):
    rows = x_ref.shape[0]
    perm = lax.broadcasted_iota(jnp.int32, (rows, rows), 0) == index_ref[...]
    o_ref[...] = dot(jnp.where(perm, 1.0, 0.0).astype(BF), x_ref[...]).astype(BF)


def expert_kernel(first, x_ref, gate_ref, up_ref, down_ref, o_ref, hidden):
    step = pl.program_id(0)

    @pl.when(step < first)
    def _():
        x = x_ref[...]
        tile = gate_ref.shape[1]
        here = pl.ds(pl.multiple_of(step * tile, tile), tile)
        hidden[:, here] = (silu(dot(x, gate_ref[...])) * dot(x, up_ref[...])).astype(BF)

    @pl.when(step >= first)
    def _():
        o_ref[...] = dot(hidden[...], down_ref[...]).reshape(o_ref.shape).astype(BF)


def combine_kernel(rows_ref, routes_ref, group_ref, pair_ref, cols_ref, o_ref):
    tokens = routes_ref.shape[0]
    ids = cols_ref[0:1, :]
    slots = cols_ref[1:2, :].astype(F32)
    weight = group_ref[...] * pair_ref[...]
    first = routes_ref[:, 0:1] == ids
    second = routes_ref[:, 1:2] == ids
    named = jnp.where(first | second, 1.0, 0.0).astype(BF)
    before = lax.broadcasted_iota(jnp.int32, (tokens, tokens), 1) < lax.broadcasted_iota(
        jnp.int32, (tokens, tokens), 0
    )
    rank = dot(jnp.where(before, 1.0, 0.0).astype(BF), named)
    mix = jnp.where(first, weight[:, 0:1], 0.0) + jnp.where(second, weight[:, 1:2], 0.0)
    mix = jnp.where(rank == slots, mix, 0.0)
    high = mix.astype(BF)
    low = (mix - high.astype(F32)).astype(BF)
    rows = rows_ref[...].reshape(ids.shape[1], rows_ref.shape[2])
    o_ref[...] = (dot(high, rows) + dot(low, rows)).astype(BF)


def project_kernel(*refs):
    *ins, o_hbm, w_hbm, lhs, wq, wk, wv, wg, w_ref, o_ref, sems, out_sems = refs
    weights = begin(sems, *zip(ins[6:], (wq, wk, wv, wg)), *rows_of(lhs, ins[:6]))
    finish(weights[:4])
    lower = 0
    for part in (wq, wk, wv, wg):
        w_ref[:, lower : lower + part.shape[1]] = part[...]
        lower += part.shape[1]
    joined = begin(out_sems, (w_ref, w_hbm))
    finish(weights[4:])
    o_ref[...] = dot(lhs[...], w_ref[...]).astype(BF)
    fetch(sems, (o_ref, o_hbm))
    finish(joined)


def split_total(total, like):
    high = total.astype(BF).astype(F32)
    mid = (total - high).astype(BF).astype(F32)
    low = total - high - mid
    row = lax.broadcasted_iota(jnp.int32, like, 0)
    return jnp.where(row == 0, high, jnp.where(row == 1, mid, low)).astype(BF)


def prefix_sums(rows):
    n = rows.shape[1]
    upper = lax.broadcasted_iota(jnp.int32, (n, n), 0) <= lax.broadcasted_iota(jnp.int32, (n, n), 1)
    return lax.dot_general(
        rows, jnp.where(upper, 1.0, 0.0), (((1,), (0,)), ((), ())),
        precision=lax.Precision.HIGHEST, preferred_element_type=F32,
    )


AWAY = (0, 3, 1, 2)


def mixer_kernel(
    me_ref, early_hbm, b0, b1, b2, b3, w_hbm, cos_hbm, sin_hbm, cos0, sin0, decay,
    g_hbm, state_ref, local_hbm, scaled_hbm,
    lhs, buf, early_ref, w_ref, cos_ref, sin_ref, cos0_ref, sin0_ref, decay_ref, steps_ref,
    local_ref, scaled_ref, g_ref, sems, late_sems,
):
    first = begin(sems, (w_hbm, w_ref), *rows_of(lhs, (b0, b1, b2, b3)))
    second = begin(
        late_sems,
        (early_hbm, early_ref),
        (cos_hbm, cos_ref),
        (sin_hbm, sin_ref),
        (cos0, cos0_ref),
        (sin0, sin0_ref),
        (decay, decay_ref),
    )
    segment, mine = me_ref[0], me_ref[1]
    y, core = mine // 2, mine % 2
    rows = 2 * b0.shape[0]
    finish(first)
    late = dot(lhs[...], w_ref[...]).astype(BF)
    finish(second)
    early = early_ref.shape[0] // rows
    for i in range(early + 2):
        owner = (y + AWAY[i // 2]) % 4 * 2 + (core + i) % 2
        here = pl.ds(pl.multiple_of(owner * rows, rows), rows)
        if i < early:
            buf[here, :] = early_ref[i * rows : (i + 1) * rows, :]
        else:
            buf[here, :] = late[(i - early) * rows : (i - early + 1) * rows, :]
    g_ref[...] = buf[:, 2 * KEY_DIM + VALUE_DIM :]

    steps_ref[...] = jnp.zeros(steps_ref.shape, F32)
    for i in range(buf.shape[0] // CHUNK):
        steps_ref[i : i + 1, :] = decay_ref[:, i * CHUNK : (i + 1) * CHUNK]
    sums = prefix_sums(steps_ref[...])
    start_cos = cos0_ref[pl.ds(segment, 1), :]
    start_sin = sin0_ref[pl.ds(segment, 1), :]
    columns = sums.T
    causal = lax.broadcasted_iota(jnp.int32, (CHUNK, CHUNK), 0) >= lax.broadcasted_iota(
        jnp.int32, (CHUNK, CHUNK), 1
    )
    state, base = None, jnp.zeros((1, 1), F32)
    for i in range(buf.shape[0] // CHUNK):
        here = slice(i * CHUNK, (i + 1) * CHUNK)
        cosine = cos_ref[here, :] * start_cos - sin_ref[here, :] * start_sin
        sine = sin_ref[here, :] * start_cos + cos_ref[here, :] * start_sin

        def rotated(lower):
            part = buf[here, lower : lower + KEY_DIM].astype(F32)
            return (part * cosine + pltpu.roll(part, KEY_DIM // 2, 1) * sine).astype(BF)

        query, key = rotated(0), rotated(KEY_DIM)
        value = buf[here, 2 * KEY_DIM : 2 * KEY_DIM + VALUE_DIM]
        row, col = sums[i : i + 1, :], columns[:, i : i + 1]
        weight = jnp.where(causal, jnp.exp(jnp.minimum(col - row, 0.0)), 0.0)
        decayed = (dot(query, key, 1, 1) * weight).astype(BF)
        out = dot(decayed, value)
        wide = query.astype(F32)
        if state is not None:
            out = out + dot((wide * jnp.exp(col)).astype(BF), state.astype(BF))
        local_ref[here, :] = out.astype(BF)
        scaled_ref[here, :] = (wide * jnp.exp(col + base)).astype(BF)
        end = row[:, CHUNK - 1 : CHUNK]
        kept = (key.astype(F32) * jnp.exp(end - col)).astype(BF)
        update = dot(kept, value, 0, 0)
        state = update if state is None else state * jnp.exp(end) + update
        base = base + end
    state_ref[0:KEY_DIM, :] = state.astype(BF)
    state_ref[KEY_DIM:, :] = split_total(base, (8, VALUE_DIM))
    fetch(sems, (g_ref, g_hbm), (local_ref, local_hbm), (scaled_ref, scaled_hbm))


def read_payload(ref):
    tail = ref[KEY_DIM:, :].astype(F32)
    return ref[0:KEY_DIM, :].astype(F32), tail[0:1] + tail[1:2] + tail[2:3]


def before_me(pos, parts):
    state, gone = 0.0, 0.0
    for j, (own, total) in enumerate(parts):
        between = 0.0
        for i, (_, other) in enumerate(parts):
            if i != j:
                inside = (pos[i] > pos[j]) & (pos[i] < pos[0])
                between = between + jnp.where(inside, other, 0.0)
        earlier = pos[j] < pos[0]
        state = state + jnp.where(earlier, own * jnp.exp(between), 0.0)
        gone = gone + jnp.where(earlier, total, 0.0)
    return state, gone


NEAR = (0, 3, 1, 2)


def x_kernel(me_ref, p0, p1, p2, p3, prefix_ref, gone_ref, state_ref):
    pos = [(me_ref[0] + k) % 4 for k in NEAR]
    parts = [read_payload(p) for p in (p0, p1, p2, p3)]
    state, gone = before_me(pos, parts)
    prefix_ref[...] = state
    gone_ref[...] = jnp.broadcast_to(jnp.exp(gone), gone_ref.shape)
    whole, total = 0.0, 0.0
    for j, (own, mine) in enumerate(parts):
        later = 0.0
        for i, (_, other) in enumerate(parts):
            if i != j:
                later = later + jnp.where(pos[i] > pos[j], other, 0.0)
        whole = whole + own * jnp.exp(later)
        total = total + mine
    state_ref[0:KEY_DIM, :] = whole.astype(BF)
    state_ref[KEY_DIM:, :] = split_total(total, (8, VALUE_DIM))


def gated_kernel(
    me_ref, p0, p1, p2, p3, prefix_ref, gone_ref, local_ref, scaled_ref, gate_ref,
    gain_ref, own_ref, twin_ref, buf,
):
    pos = [(me_ref[0] // 4 + k) % 4 for k in NEAR]
    parts = [read_payload(p) for p in (p0, p1, p2, p3)]
    state, _ = before_me(pos, parts)
    incoming = (prefix_ref[...] + gone_ref[0:1, :] * state).astype(BF)
    retained = local_ref[...].astype(F32) + dot(scaled_ref[...], incoming)
    heads = normalised(retained, gain_ref[...])
    buf[...] = (silu(gate_ref[...].astype(F32)) * heads).astype(BF)
    core = me_ref[1] % 2
    rows = own_ref.shape[0] // 4
    for y in range(4):
        there = slice(y * rows, (y + 1) * rows)
        own_ref[there, :] = buf[pl.ds(pl.multiple_of((2 * y + core) * rows, rows), rows), :]
        twin_ref[there, :] = buf[pl.ds(pl.multiple_of((2 * y + 1 - core) * rows, rows), rows), :]


def output_kernel(me_ref, own_ref, twin_ref, wo_ref, wt_ref, o0, o1, o2, o3, lhs, lht):
    rows = o0.shape[0]
    for k in range(4):
        here = slice(k * rows, (k + 1) * rows)
        y = (me_ref[1] // 2 + (0, 1, 3, 2)[k]) % 4
        there = pl.ds(pl.multiple_of(y * rows, rows), rows)
        lhs[here, :] = own_ref[there, :]
        lht[here, :] = twin_ref[there, :]
    out = (dot(lhs[...], wo_ref[...]) + dot(lht[...], wt_ref[...])).astype(BF)
    for k, ref in enumerate((o0, o1, o2, o3)):
        ref[...] = out[k * rows : (k + 1) * rows, :]


def sum_kernel(a, b, c, d, o_ref):
    o_ref[...] = (
        a[...].astype(F32) + b[...].astype(F32) + c[...].astype(F32) + d[...].astype(F32)
    ).astype(BF)


def core_swap(x):
    return lax.ppermute(x, "tp", [(t, t ^ 1) for t in range(8)])


def y_shift(x, k):
    return lax.ppermute(x, "tp", [(t, ((t // 2 + k) % 4) * 2 + t % 2) for t in range(8)])


def x_shift(x, k):
    return lax.ppermute(x, "ep", [(e, (e // 4) * 4 + (e + k) % 4) for e in range(16)])


def z_shift(x, k):
    return lax.ppermute(x, "ep", [(e, (e + 4 * k) % 16) for e in range(16)])


def exchange(x, axis):
    return lax.all_to_all(x, axis, split_axis=0, concat_axis=0, tiled=True)


def rotation(positions):
    half = KEY_DIM // 2
    frequency = THETA ** (-np.arange(half) / half)
    angles = positions[:, None].astype(np.float64) * frequency[None, :]
    cosine, sine = np.cos(angles), np.sin(angles)
    return (
        np.concatenate([cosine, cosine], axis=1).astype(np.float32),
        np.concatenate([-sine, sine], axis=1).astype(np.float32),
    )


def local(
    mixer_input,
    log_decay,
    mixer_gain,
    query_weight,
    key_weight,
    value_weight,
    gate_weight,
    head_gain,
    output_weight,
    expert_input,
    expert_gain,
    routes,
    group_weight,
    pair_weight,
    expert_gate,
    expert_up,
    expert_down,
):
    rows, width = mixer_input.shape
    seg_rows = log_decay.shape[0]
    ep, tp = lax.axis_index("ep"), lax.axis_index("tp")
    n_ep, n_tp = lax.axis_size("ep"), lax.axis_size("tp")
    slots = n_ep * n_tp * CAP

    sems = lambda n: pltpu.SemaphoreType.DMA((n,))
    normed = run(
        norm_kernel,
        shape((rows, width)),
        (mixer_input, mixer_gain[None]),
        hbm=(0, 1),
        vmem=60 << 20,
        scratch=(pltpu.VMEM((rows, width), BF), pltpu.VMEM((1, width), F32), sems(2)),
    )
    from_below = y_shift(normed, 1)
    from_above = y_shift(normed, -1)
    twin = core_swap(normed)

    outgoing = run(
        dispatch_kernel,
        shape((n_ep, CAP, n_tp, width)),
        (after(expert_input, normed), expert_gain[None], routes.T),
        flops=2 * slots * rows * width,
        hbm=(0, 1, 2),
        vmem=60 << 20,
        scratch=(
            pltpu.VMEM((rows, width), BF),
            pltpu.VMEM((1, width), F32),
            pltpu.VMEM((2, rows), jnp.int32),
            sems(3),
        ),
    )
    staged = exchange(outgoing, "ep")

    twin_out = core_swap(output_weight)
    weights = (query_weight, key_weight, value_weight, gate_weight)
    cols = sum(w.shape[1] for w in weights)
    cosine, sine = rotation(np.arange(seg_rows))
    cosine_start, sine_start = rotation(np.arange(n_ep) * seg_rows)
    me = jnp.stack([ep, tp]).astype(jnp.int32)
    half = rows // 2
    far_low = y_shift(from_below[:half], 1)
    far_high = y_shift(from_above[half:], -1)
    below_twin, above_twin = core_swap(from_below), core_swap(from_above)
    early, joined = run(
        project_kernel,
        (shape((6 * rows, cols)), shape((width, cols))),
        (
            after(normed, me),
            twin, from_below, below_twin, from_above, above_twin,
            *weights,
        ),
        flops=2 * 6 * rows * width * cols,
        hbm=range(10),
        hbm_outs=(0, 1),
        vmem=60 << 20,
        scratch=(
            pltpu.VMEM((6 * rows, width), BF),
            *(pltpu.VMEM(w.shape, BF) for w in weights),
            pltpu.VMEM((width, cols), BF),
            pltpu.VMEM((6 * rows, cols), BF),
            sems(10),
            sems(1),
        ),
    )
    low_twin, high_twin = core_swap(far_low), core_swap(far_high)
    gate, state, local_out, scaled = run(
        mixer_kernel,
        (
            shape((seg_rows, VALUE_DIM)),
            shape((KEY_DIM + 8, VALUE_DIM)),
            shape((seg_rows, VALUE_DIM)),
            shape((seg_rows, KEY_DIM)),
        ),
        (
            me, early, far_low, far_high, low_twin, high_twin, joined,
            cosine, sine, cosine_start, sine_start, log_decay.T,
        ),
        scalars=1,
        flops=2 * 2 * rows * width * cols,
        hbm=range(1, 12),
        hbm_outs=(0, 2, 3),
        vmem=60 << 20,
        scratch=(
            pltpu.VMEM((2 * rows, width), BF),
            pltpu.VMEM((seg_rows, cols), BF),
            pltpu.VMEM((6 * rows, cols), BF),
            pltpu.VMEM((width, cols), BF),
            pltpu.VMEM((seg_rows, KEY_DIM), F32),
            pltpu.VMEM((seg_rows, KEY_DIM), F32),
            pltpu.VMEM((n_ep, KEY_DIM), F32),
            pltpu.VMEM((n_ep, KEY_DIM), F32),
            pltpu.VMEM((1, seg_rows), F32),
            pltpu.VMEM((8, CHUNK), F32),
            pltpu.VMEM((seg_rows, VALUE_DIM), BF),
            pltpu.VMEM((seg_rows, KEY_DIM), BF),
            pltpu.VMEM((seg_rows, VALUE_DIM), BF),
            sems(5),
            sems(6),
        ),
    )

    index = jnp.arange(slots, dtype=jnp.int32)
    deep = n_ep * CAP
    to_tp = ((index % n_tp) * deep + index // n_tp)[None]
    turned = run(
        turn_kernel,
        shape((slots, width)),
        (to_tp, after(staged, state).reshape(slots, width)),
        flops=2 * slots * slots * width,
    )
    tokens = exchange(turned.reshape(n_tp, deep, width), "tp").reshape(slots, width)

    payloads = (state, x_shift(state, 1), x_shift(state, -1), x_shift(state, 2))
    prefix, gone, plane = run(
        x_kernel,
        (
            shape((KEY_DIM, VALUE_DIM), F32),
            shape((8, VALUE_DIM), F32),
            shape((KEY_DIM + 8, VALUE_DIM)),
        ),
        (me, *payloads),
        scalars=1,
    )
    planes = (plane, z_shift(plane, 1), z_shift(plane, -1), z_shift(plane, 2))
    own_gated, twin_gated = run(
        gated_kernel,
        (shape((4 * rows, VALUE_DIM)), shape((4 * rows, VALUE_DIM))),
        (me, *planes, prefix, gone, local_out, scaled, gate, head_gain[None]),
        scalars=1,
        flops=2 * seg_rows * KEY_DIM * VALUE_DIM,
        scratch=(pltpu.VMEM((seg_rows, VALUE_DIM), BF),),
    )
    inner = expert_gate.shape[2]
    tile, wide = 512, 1024
    first = inner // tile
    experts = pl.pallas_call(
        functools.partial(expert_kernel, first),
        grid=(first + width // wide,),
        out_shape=shape((n_ep * n_tp, CAP, width)),
        in_specs=[
            pl.BlockSpec((slots, width), lambda f: (0, 0)),
            pl.BlockSpec((width, tile), lambda f: (0, jnp.minimum(f, first - 1))),
            pl.BlockSpec((width, tile), lambda f: (0, jnp.minimum(f, first - 1))),
            pl.BlockSpec((inner, wide), lambda f: (0, jnp.maximum(f - first, 0))),
        ],
        out_specs=pl.BlockSpec(
            (n_ep * n_tp, CAP, wide), lambda f: (0, 0, jnp.maximum(f - first, 0))
        ),
        scratch_shapes=[pltpu.VMEM((slots, inner), BF)],
        compiler_params=pltpu.CompilerParams(
            vmem_limit_bytes=60 << 20, dimension_semantics=("arbitrary",)
        ),
        cost_estimate=pl.CostEstimate(
            flops=6 * slots * width * inner, bytes_accessed=6 * width * inner, transcendentals=0
        ),
    )
    other_gated = core_swap(twin_gated)
    kept, up, down, far = run(
        output_kernel,
        tuple(shape((rows, width)) for _ in range(4)),
        (me, own_gated, other_gated, output_weight, twin_out),
        scalars=1,
        flops=2 * 4 * rows * 2 * VALUE_DIM * width,
        scratch=(pltpu.VMEM((4 * rows, VALUE_DIM), BF), pltpu.VMEM((4 * rows, VALUE_DIM), BF)),
    )
    got_up = y_shift(up, 1)
    got_down = y_shift(down, -1)
    got_far = y_shift(far, 2)
    results = experts(after(tokens, kept), expert_gate[0], expert_up[0], expert_down[0])
    mixer_output = run(sum_kernel, shape((rows, width)), (kept, got_up, got_down, got_far))

    returned = exchange(results, ("tp", "ep"))
    columns = jnp.stack([index % deep // CAP * n_tp + index // deep, index % CAP])
    expert_output = run(
        combine_kernel,
        shape((rows, width)),
        (returned, routes, group_weight[:, None], pair_weight, columns),
        flops=4 * slots * rows * width,
    )
    return (mixer_output, expert_output)


def solution(mesh):
    both = ("ep", "tp")
    return jax.shard_map(
        local,
        mesh=mesh,
        in_specs=(
            P(both, None),
            P("ep", "tp"),
            P(),
            P(None, "tp"),
            P(None, "tp"),
            P(None, "tp"),
            P(None, "tp"),
            P("tp"),
            P("tp", None),
            P(both, None),
            P(),
            P(both, None),
            P(both),
            P(both, None),
            P(both, None, None),
            P(both, None, None),
            P(both, None, None),
        ),
        out_specs=(P(both, None), P(both, None)),
        check_vma=False,
    )
```

```python
import functools

import jax
import jax.numpy as jnp
import numpy as np
from jax import lax
from jax.experimental import pallas as pl
from jax.experimental.pallas import tpu as pltpu
from jax.sharding import PartitionSpec as P


KEY_DIM = 128
VALUE_DIM = 256
CHUNK = 256
CAP = 3
EPSILON = 1e-05
THETA = 10000.0
BF = jnp.bfloat16
F32 = jnp.float32
VM = pl.BlockSpec(memory_space=pltpu.VMEM)
SM = pl.BlockSpec(memory_space=pltpu.SMEM)


HBM = pl.BlockSpec(memory_space=pltpu.HBM)


def run(kernel, outs, args, scalars=0, flops=0, scratch=(), vmem=24 << 20, hbm=(), hbm_outs=()):
    nbytes = sum(a.size * a.dtype.itemsize for a in args) + sum(
        o.size * o.dtype.itemsize for o in jax.tree.leaves(outs)
    )
    return pl.pallas_call(
        kernel,
        out_shape=outs,
        in_specs=[SM if i < scalars else HBM if i in hbm else VM for i in range(len(args))],
        out_specs=tuple(HBM if i in hbm_outs else VM for i in range(len(outs)))
        if isinstance(outs, tuple)
        else VM,
        scratch_shapes=list(scratch),
        compiler_params=pltpu.CompilerParams(vmem_limit_bytes=vmem),
        cost_estimate=pl.CostEstimate(flops=flops, bytes_accessed=nbytes, transcendentals=0),
    )(*args)


def after(value, *earlier):
    return lax.optimization_barrier((value, *earlier))[0]


def shape(dims, dtype=BF):
    return jax.ShapeDtypeStruct(dims, dtype)


def dot(a, b, ca=1, cb=0):
    return lax.dot_general(a, b, (((ca,), (cb,)), ((), ())), preferred_element_type=F32)


def silu(v):
    return v * (1.0 / (1.0 + jnp.exp(-v)))


def normalised(x, gain):
    x = x.astype(F32)
    centred = x - jnp.mean(x, axis=-1, keepdims=True)
    spread = jnp.mean(centred * centred, axis=-1, keepdims=True)
    return centred * lax.rsqrt(spread + EPSILON) * gain


def begin(sems, *pairs):
    copies = [pltpu.make_async_copy(a, b, sems.at[i]) for i, (a, b) in enumerate(pairs)]
    for copy in copies:
        copy.start()
    return copies


def finish(copies):
    for copy in copies:
        copy.wait()


def fetch(sems, *pairs):
    finish(begin(sems, *pairs))


def rows_of(ref, parts):
    pairs, lower = [], 0
    for part in parts:
        pairs.append((part, ref.at[lower : lower + part.shape[0], :]))
        lower += part.shape[0]
    return pairs


def norm_kernel(x_hbm, gain_hbm, o_ref, x_ref, gain_ref, sems):
    fetch(sems, (x_hbm, x_ref), (gain_hbm, gain_ref))
    o_ref[...] = normalised(x_ref[...], gain_ref[...]).astype(BF)


def dispatch_kernel(x_hbm, gain_hbm, routes_hbm, o_ref, x_ref, gain_ref, routes_ref, sems):
    fetch(sems, (x_hbm, x_ref), (gain_hbm, gain_ref), (routes_hbm, routes_ref))
    rows = normalised(x_ref[...], gain_ref[...]).astype(BF)
    tokens = rows.shape[0]
    experts = o_ref.shape[0] * o_ref.shape[2]
    ids = lax.broadcasted_iota(jnp.int32, (experts, tokens), 0)
    named = (ids == routes_ref[0:1, :]) | (ids == routes_ref[1:2, :])
    named = jnp.where(named, 1.0, 0.0)
    before = lax.broadcasted_iota(jnp.int32, (tokens, tokens), 0) < lax.broadcasted_iota(
        jnp.int32, (tokens, tokens), 1
    )
    rank = dot(named.astype(BF), jnp.where(before, 1.0, 0.0).astype(BF))
    for slot in range(CAP):
        pick = jnp.where(rank == float(slot), named, 0.0).astype(BF)
        o_ref[:, slot] = dot(pick, rows).astype(BF).reshape(
            o_ref.shape[0], o_ref.shape[2], o_ref.shape[3]
        )


def turn_kernel(index_ref, x_ref, o_ref):
    rows = x_ref.shape[0]
    perm = lax.broadcasted_iota(jnp.int32, (rows, rows), 0) == index_ref[...]
    o_ref[...] = dot(jnp.where(perm, 1.0, 0.0).astype(BF), x_ref[...]).astype(BF)


def expert_kernel(first, x_ref, gate_ref, up_ref, down_ref, o_ref, hidden):
    step = pl.program_id(0)

    @pl.when(step < first)
    def _():
        x = x_ref[...]
        tile = gate_ref.shape[1]
        here = pl.ds(pl.multiple_of(step * tile, tile), tile)
        hidden[:, here] = (silu(dot(x, gate_ref[...])) * dot(x, up_ref[...])).astype(BF)

    @pl.when(step >= first)
    def _():
        o_ref[...] = dot(hidden[...], down_ref[...]).reshape(o_ref.shape).astype(BF)


def mix_kernel(routes_ref, group_ref, pair_ref, cols_ref, high_ref, low_ref):
    tokens = routes_ref.shape[0]
    ids = cols_ref[0:1, :]
    slots = cols_ref[1:2, :].astype(F32)
    weight = group_ref[...] * pair_ref[...]
    first = routes_ref[:, 0:1] == ids
    second = routes_ref[:, 1:2] == ids
    named = jnp.where(first | second, 1.0, 0.0).astype(BF)
    before = lax.broadcasted_iota(jnp.int32, (tokens, tokens), 1) < lax.broadcasted_iota(
        jnp.int32, (tokens, tokens), 0
    )
    rank = dot(jnp.where(before, 1.0, 0.0).astype(BF), named)
    mix = jnp.where(first, weight[:, 0:1], 0.0) + jnp.where(second, weight[:, 1:2], 0.0)
    mix = jnp.where(rank == slots, mix, 0.0)
    high = mix.astype(BF)
    high_ref[...] = high
    low_ref[...] = (mix - high.astype(F32)).astype(BF)


def combine_kernel(rows_ref, high_ref, low_ref, o_ref):
    rows = rows_ref[...].reshape(high_ref.shape[1], rows_ref.shape[2])
    o_ref[...] = (dot(high_ref[...], rows) + dot(low_ref[...], rows)).astype(BF)


def project_kernel(*refs):
    *ins, o_hbm, w_hbm, lhs, wq, wk, wv, wg, w_ref, o_ref, sems, out_sems = refs
    weights = begin(sems, *zip(ins[6:], (wq, wk, wv, wg)), *rows_of(lhs, ins[:6]))
    finish(weights[:4])
    lower = 0
    for part in (wq, wk, wv, wg):
        w_ref[:, lower : lower + part.shape[1]] = part[...]
        lower += part.shape[1]
    joined = begin(out_sems, (w_ref, w_hbm))
    finish(weights[4:])
    o_ref[...] = dot(lhs[...], w_ref[...]).astype(BF)
    fetch(sems, (o_ref, o_hbm))
    finish(joined)


def split_total(total, like):
    high = total.astype(BF).astype(F32)
    mid = (total - high).astype(BF).astype(F32)
    low = total - high - mid
    row = lax.broadcasted_iota(jnp.int32, like, 0)
    return jnp.where(row == 0, high, jnp.where(row == 1, mid, low)).astype(BF)


def prefix_sums(rows):
    n = rows.shape[1]
    upper = lax.broadcasted_iota(jnp.int32, (n, n), 0) <= lax.broadcasted_iota(jnp.int32, (n, n), 1)
    return lax.dot_general(
        rows, jnp.where(upper, 1.0, 0.0), (((1,), (0,)), ((), ())),
        precision=lax.Precision.HIGHEST, preferred_element_type=F32,
    )


AWAY = (0, 3, 1, 2)


def chunk_sums(decay_ref, steps_ref):
    steps_ref[...] = jnp.zeros(steps_ref.shape, F32)
    for i in range(decay_ref.shape[1] // CHUNK):
        steps_ref[i : i + 1, :] = decay_ref[:, i * CHUNK : (i + 1) * CHUNK]
    return prefix_sums(steps_ref[...])


def mixer_kernel(
    me_ref, early_hbm, b0, b1, b2, b3, w_hbm, cos_hbm, sin_hbm, cos0, sin0, decay,
    g_hbm, state_ref, q_hbm, k_hbm, v_hbm,
    lhs, buf, early_ref, w_ref, cos_ref, sin_ref, cos0_ref, sin0_ref, decay_ref, steps_ref,
    q_ref, k_ref, v_ref, g_ref, kept_ref, sems, late_sems,
):
    second = begin(
        late_sems,
        (decay, decay_ref),
        (early_hbm, early_ref),
        (cos_hbm, cos_ref),
        (sin_hbm, sin_ref),
        (cos0, cos0_ref),
        (sin0, sin0_ref),
    )
    first = begin(sems, (w_hbm, w_ref))
    segment, mine = me_ref[0], me_ref[1]
    y, core = mine // 2, mine % 2
    rows = 2 * b0.shape[0]
    early = early_ref.shape[0] // rows

    def placed(i, block):
        owner = (y + AWAY[i // 2]) % 4 * 2 + (core + i) % 2
        buf[pl.ds(pl.multiple_of(owner * rows, rows), rows), :] = block

    finish(second)
    sums = chunk_sums(decay_ref, steps_ref)
    columns = sums.T
    chunks = buf.shape[0] // CHUNK
    ends = [sums[i : i + 1, CHUNK - 1 : CHUNK] for i in range(chunks)]
    remain, total = [], jnp.zeros((1, 1), F32)
    for i in reversed(range(chunks)):
        remain.append(jnp.exp(total + ends[i] - columns[:, i : i + 1]))
        total = total + ends[i]
    remain = remain[::-1]
    start_cos = cos0_ref[pl.ds(segment, 1), :]
    start_sin = sin0_ref[pl.ds(segment, 1), :]
    for i in range(early):
        placed(i, early_ref[i * rows : (i + 1) * rows, :])
    for block, there in rows_of(lhs, (b0, b1, b2, b3)):
        there[...] = block[...]
    finish(first)
    late = dot(lhs[...], w_ref[...]).astype(BF)
    for i in range(2):
        placed(early + i, late[i * rows : (i + 1) * rows, :])
    v_ref[...] = buf[:, 2 * KEY_DIM : 2 * KEY_DIM + VALUE_DIM]
    g_ref[...] = buf[:, 2 * KEY_DIM + VALUE_DIM :]
    for i in range(chunks):
        here = slice(i * CHUNK, (i + 1) * CHUNK)
        cosine = cos_ref[here, :] * start_cos - sin_ref[here, :] * start_sin
        sine = sin_ref[here, :] * start_cos + cos_ref[here, :] * start_sin

        def rotated(lower):
            part = buf[here, lower : lower + KEY_DIM].astype(F32)
            return (part * cosine + pltpu.roll(part, KEY_DIM // 2, 1) * sine).astype(BF)

        key = rotated(KEY_DIM)
        k_ref[here, :] = key
        kept_ref[here, :] = (key.astype(F32) * remain[i]).astype(BF)
        q_ref[here, :] = rotated(0)
    copies = begin(late_sems, (q_ref, q_hbm), (k_ref, k_hbm), (v_ref, v_hbm), (g_ref, g_hbm))
    state_ref[0:KEY_DIM, :] = dot(kept_ref[...], v_ref[...], 0, 0).astype(BF)
    state_ref[KEY_DIM:, :] = split_total(total, (8, VALUE_DIM))
    finish(copies)


def retain_kernel(
    q_hbm, k_hbm, v_hbm, decay, local_ref, scaled_ref,
    q_ref, k_ref, v_ref, decay_ref, steps_ref, sems,
):
    copies = begin(sems, (decay, decay_ref), (q_hbm, q_ref), (k_hbm, k_ref), (v_hbm, v_ref))
    causal = lax.broadcasted_iota(jnp.int32, (CHUNK, CHUNK), 0) >= lax.broadcasted_iota(
        jnp.int32, (CHUNK, CHUNK), 1
    )
    finish(copies)
    sums = chunk_sums(decay_ref, steps_ref)
    columns = sums.T
    state, base = None, jnp.zeros((1, 1), F32)
    chunks = q_ref.shape[0] // CHUNK
    for i in range(chunks):
        here = slice(i * CHUNK, (i + 1) * CHUNK)
        query, key, value = q_ref[here, :], k_ref[here, :], v_ref[here, :]
        row, col = sums[i : i + 1, :], columns[:, i : i + 1]
        weight = jnp.where(causal, jnp.exp(jnp.minimum(col - row, 0.0)), 0.0)
        decayed = (dot(query, key, 1, 1) * weight).astype(BF)
        out = dot(decayed, value)
        wide = query.astype(F32)
        if state is not None:
            out = out + dot((wide * jnp.exp(col)).astype(BF), state.astype(BF))
        local_ref[here, :] = out.astype(BF)
        scaled_ref[here, :] = (wide * jnp.exp(col + base)).astype(BF)
        end = row[:, CHUNK - 1 : CHUNK]
        if i < chunks - 1:
            kept = (key.astype(F32) * jnp.exp(end - col)).astype(BF)
            update = dot(kept, value, 0, 0)
            state = update if state is None else state * jnp.exp(end) + update
        base = base + end


def read_payload(ref):
    tail = ref[KEY_DIM:, :].astype(F32)
    return ref[0:KEY_DIM, :].astype(F32), tail[0:1] + tail[1:2] + tail[2:3]


def before_me(pos, parts):
    state, gone = 0.0, 0.0
    for j, (own, total) in enumerate(parts):
        between = 0.0
        for i, (_, other) in enumerate(parts):
            if i != j:
                inside = (pos[i] > pos[j]) & (pos[i] < pos[0])
                between = between + jnp.where(inside, other, 0.0)
        earlier = pos[j] < pos[0]
        state = state + jnp.where(earlier, own * jnp.exp(between), 0.0)
        gone = gone + jnp.where(earlier, total, 0.0)
    return state, gone


NEAR = (0, 3, 1, 2)


def x_kernel(me_ref, p0, p1, p2, p3, prefix_ref, gone_ref, state_ref):
    pos = [(me_ref[0] + k) % 4 for k in NEAR]
    parts = [read_payload(p) for p in (p0, p1, p2, p3)]
    state, gone = before_me(pos, parts)
    prefix_ref[...] = state
    gone_ref[...] = jnp.broadcast_to(jnp.exp(gone), gone_ref.shape)
    whole, total = 0.0, 0.0
    for j, (own, mine) in enumerate(parts):
        later = 0.0
        for i, (_, other) in enumerate(parts):
            if i != j:
                later = later + jnp.where(pos[i] > pos[j], other, 0.0)
        whole = whole + own * jnp.exp(later)
        total = total + mine
    state_ref[0:KEY_DIM, :] = whole.astype(BF)
    state_ref[KEY_DIM:, :] = split_total(total, (8, VALUE_DIM))


def gated_kernel(
    me_ref, p0, p1, p2, p3, prefix_ref, gone_ref, local_ref, scaled_ref, gate_ref,
    gain_ref, own_ref, twin_ref, buf,
):
    pos = [(me_ref[0] // 4 + k) % 4 for k in NEAR]
    parts = [read_payload(p) for p in (p0, p1, p2, p3)]
    state, _ = before_me(pos, parts)
    incoming = (prefix_ref[...] + gone_ref[0:1, :] * state).astype(BF)
    retained = local_ref[...].astype(F32) + dot(scaled_ref[...], incoming)
    heads = normalised(retained, gain_ref[...])
    buf[...] = (silu(gate_ref[...].astype(F32)) * heads).astype(BF)
    core = me_ref[1] % 2
    rows = own_ref.shape[0] // 4
    for y in range(4):
        there = slice(y * rows, (y + 1) * rows)
        own_ref[there, :] = buf[pl.ds(pl.multiple_of((2 * y + core) * rows, rows), rows), :]
        twin_ref[there, :] = buf[pl.ds(pl.multiple_of((2 * y + 1 - core) * rows, rows), rows), :]


def output_kernel(me_ref, own_ref, twin_ref, wo_ref, wt_ref, o0, o1, o2, o3, lhs, lht):
    rows = o0.shape[0]
    for k in range(4):
        here = slice(k * rows, (k + 1) * rows)
        y = (me_ref[1] // 2 + (0, 1, 3, 2)[k]) % 4
        there = pl.ds(pl.multiple_of(y * rows, rows), rows)
        lhs[here, :] = own_ref[there, :]
        lht[here, :] = twin_ref[there, :]
    out = (dot(lhs[...], wo_ref[...]) + dot(lht[...], wt_ref[...])).astype(BF)
    for k, ref in enumerate((o0, o1, o2, o3)):
        ref[...] = out[k * rows : (k + 1) * rows, :]


def sum_kernel(a, b, c, d, o_ref):
    o_ref[...] = (
        a[...].astype(F32) + b[...].astype(F32) + c[...].astype(F32) + d[...].astype(F32)
    ).astype(BF)


def core_swap(x):
    return lax.ppermute(x, "tp", [(t, t ^ 1) for t in range(8)])


def y_shift(x, k):
    return lax.ppermute(x, "tp", [(t, ((t // 2 + k) % 4) * 2 + t % 2) for t in range(8)])


def x_shift(x, k):
    return lax.ppermute(x, "ep", [(e, (e // 4) * 4 + (e + k) % 4) for e in range(16)])


def z_shift(x, k):
    return lax.ppermute(x, "ep", [(e, (e + 4 * k) % 16) for e in range(16)])


def exchange(x, axis):
    return lax.all_to_all(x, axis, split_axis=0, concat_axis=0, tiled=True)


def rotation(positions):
    half = KEY_DIM // 2
    frequency = THETA ** (-np.arange(half) / half)
    angles = positions[:, None].astype(np.float64) * frequency[None, :]
    cosine, sine = np.cos(angles), np.sin(angles)
    return (
        np.concatenate([cosine, cosine], axis=1).astype(np.float32),
        np.concatenate([-sine, sine], axis=1).astype(np.float32),
    )


def local(
    mixer_input,
    log_decay,
    mixer_gain,
    query_weight,
    key_weight,
    value_weight,
    gate_weight,
    head_gain,
    output_weight,
    expert_input,
    expert_gain,
    routes,
    group_weight,
    pair_weight,
    expert_gate,
    expert_up,
    expert_down,
):
    rows, width = mixer_input.shape
    seg_rows = log_decay.shape[0]
    ep, tp = lax.axis_index("ep"), lax.axis_index("tp")
    n_ep, n_tp = lax.axis_size("ep"), lax.axis_size("tp")
    slots = n_ep * n_tp * CAP
    me = jnp.stack([ep, tp]).astype(jnp.int32)

    sems = lambda n: pltpu.SemaphoreType.DMA((n,))
    normed = run(
        norm_kernel,
        shape((rows, width)),
        (mixer_input, mixer_gain[None]),
        hbm=(0, 1),
        vmem=60 << 20,
        scratch=(pltpu.VMEM((rows, width), BF), pltpu.VMEM((1, width), F32), sems(2)),
    )
    from_below = y_shift(normed, 1)
    from_above = y_shift(normed, -1)
    twin = core_swap(normed)

    outgoing = run(
        dispatch_kernel,
        shape((n_ep, CAP, n_tp, width)),
        (after(expert_input, normed, me), expert_gain[None], routes.T),
        flops=2 * slots * rows * width,
        hbm=(0, 1, 2),
        vmem=60 << 20,
        scratch=(
            pltpu.VMEM((rows, width), BF),
            pltpu.VMEM((1, width), F32),
            pltpu.VMEM((2, rows), jnp.int32),
            sems(3),
        ),
    )
    staged = exchange(outgoing, "ep")

    twin_out = core_swap(output_weight)
    weights = (query_weight, key_weight, value_weight, gate_weight)
    cols = sum(w.shape[1] for w in weights)
    cosine, sine = rotation(np.arange(seg_rows))
    cosine_start, sine_start = rotation(np.arange(n_ep) * seg_rows)
    half = rows // 2
    far_low = y_shift(from_below[:half], 1)
    far_high = y_shift(from_above[half:], -1)
    below_twin, above_twin = core_swap(from_below), core_swap(from_above)
    early, joined = run(
        project_kernel,
        (shape((6 * rows, cols)), shape((width, cols))),
        (
            normed,
            twin, from_below, below_twin, from_above, above_twin,
            *weights,
        ),
        flops=2 * 6 * rows * width * cols,
        hbm=range(10),
        hbm_outs=(0, 1),
        vmem=60 << 20,
        scratch=(
            pltpu.VMEM((6 * rows, width), BF),
            *(pltpu.VMEM(w.shape, BF) for w in weights),
            pltpu.VMEM((width, cols), BF),
            pltpu.VMEM((6 * rows, cols), BF),
            sems(10),
            sems(1),
        ),
    )
    low_twin, high_twin = core_swap(far_low), core_swap(far_high)
    gate, state, query, key, value = run(
        mixer_kernel,
        (
            shape((seg_rows, VALUE_DIM)),
            shape((KEY_DIM + 8, VALUE_DIM)),
            shape((seg_rows, KEY_DIM)),
            shape((seg_rows, KEY_DIM)),
            shape((seg_rows, VALUE_DIM)),
        ),
        (
            me, early, far_low, far_high, low_twin, high_twin, joined,
            cosine, sine, cosine_start, sine_start, log_decay.T,
        ),
        scalars=1,
        flops=2 * 2 * rows * width * cols,
        hbm=(1, 6, 7, 8, 9, 10, 11),
        hbm_outs=(0, 2, 3, 4),
        vmem=60 << 20,
        scratch=(
            pltpu.VMEM((2 * rows, width), BF),
            pltpu.VMEM((seg_rows, cols), BF),
            pltpu.VMEM((6 * rows, cols), BF),
            pltpu.VMEM((width, cols), BF),
            pltpu.VMEM((seg_rows, KEY_DIM), F32),
            pltpu.VMEM((seg_rows, KEY_DIM), F32),
            pltpu.VMEM((n_ep, KEY_DIM), F32),
            pltpu.VMEM((n_ep, KEY_DIM), F32),
            pltpu.VMEM((1, seg_rows), F32),
            pltpu.VMEM((8, CHUNK), F32),
            pltpu.VMEM((seg_rows, KEY_DIM), BF),
            pltpu.VMEM((seg_rows, KEY_DIM), BF),
            pltpu.VMEM((seg_rows, VALUE_DIM), BF),
            pltpu.VMEM((seg_rows, VALUE_DIM), BF),
            pltpu.VMEM((seg_rows, KEY_DIM), BF),
            sems(5),
            sems(6),
        ),
    )

    index = jnp.arange(slots, dtype=jnp.int32)
    deep = n_ep * CAP
    to_tp = ((index % n_tp) * deep + index // n_tp)[None]
    turned = run(
        turn_kernel,
        shape((slots, width)),
        (to_tp, after(staged, state).reshape(slots, width)),
        flops=2 * slots * slots * width,
    )
    tokens = exchange(turned.reshape(n_tp, deep, width), "tp").reshape(slots, width)

    payloads = (state, x_shift(state, 1), x_shift(state, -1), x_shift(state, 2))
    prefix, gone, plane = run(
        x_kernel,
        (
            shape((KEY_DIM, VALUE_DIM), F32),
            shape((8, VALUE_DIM), F32),
            shape((KEY_DIM + 8, VALUE_DIM)),
        ),
        (me, *payloads),
        scalars=1,
    )
    planes = (plane, z_shift(plane, 1), z_shift(plane, -1), z_shift(plane, 2))
    local_out, scaled = run(
        retain_kernel,
        (shape((seg_rows, VALUE_DIM)), shape((seg_rows, KEY_DIM))),
        (query, key, value, log_decay.T),
        flops=8 * seg_rows * CHUNK * VALUE_DIM,
        hbm=range(4),
        scratch=(
            pltpu.VMEM((seg_rows, KEY_DIM), BF),
            pltpu.VMEM((seg_rows, KEY_DIM), BF),
            pltpu.VMEM((seg_rows, VALUE_DIM), BF),
            pltpu.VMEM((1, seg_rows), F32),
            pltpu.VMEM((8, CHUNK), F32),
            sems(4),
        ),
    )
    own_gated, twin_gated = run(
        gated_kernel,
        (shape((4 * rows, VALUE_DIM)), shape((4 * rows, VALUE_DIM))),
        (me, *planes, prefix, gone, local_out, scaled, gate, head_gain[None]),
        scalars=1,
        flops=2 * seg_rows * KEY_DIM * VALUE_DIM,
        scratch=(pltpu.VMEM((seg_rows, VALUE_DIM), BF),),
    )
    inner = expert_gate.shape[2]
    tile, wide = 512, 1024
    first = inner // tile
    experts = pl.pallas_call(
        functools.partial(expert_kernel, first),
        grid=(first + width // wide,),
        out_shape=shape((n_ep * n_tp, CAP, width)),
        in_specs=[
            pl.BlockSpec((slots, width), lambda f: (0, 0)),
            pl.BlockSpec((width, tile), lambda f: (0, jnp.minimum(f, first - 1))),
            pl.BlockSpec((width, tile), lambda f: (0, jnp.minimum(f, first - 1))),
            pl.BlockSpec((inner, wide), lambda f: (0, jnp.maximum(f - first, 0))),
        ],
        out_specs=pl.BlockSpec(
            (n_ep * n_tp, CAP, wide), lambda f: (0, 0, jnp.maximum(f - first, 0))
        ),
        scratch_shapes=[pltpu.VMEM((slots, inner), BF)],
        compiler_params=pltpu.CompilerParams(
            vmem_limit_bytes=60 << 20, dimension_semantics=("arbitrary",)
        ),
        cost_estimate=pl.CostEstimate(
            flops=6 * slots * width * inner, bytes_accessed=6 * width * inner, transcendentals=0
        ),
    )
    other_gated = core_swap(twin_gated)
    kept, up, down, far = run(
        output_kernel,
        tuple(shape((rows, width)) for _ in range(4)),
        (me, own_gated, other_gated, output_weight, twin_out),
        scalars=1,
        flops=2 * 4 * rows * 2 * VALUE_DIM * width,
        scratch=(pltpu.VMEM((4 * rows, VALUE_DIM), BF), pltpu.VMEM((4 * rows, VALUE_DIM), BF)),
    )
    got_up = y_shift(up, 1)
    got_down = y_shift(down, -1)
    got_far = y_shift(far, 2)
    results = experts(after(tokens, kept), expert_gate[0], expert_up[0], expert_down[0])
    mixer_output = run(sum_kernel, shape((rows, width)), (kept, got_up, got_down, got_far))

    returned = exchange(results, ("tp", "ep"))
    columns = jnp.stack([index % deep // CAP * n_tp + index // deep, index % CAP])
    high, low = run(
        mix_kernel,
        (shape((rows, slots)), shape((rows, slots))),
        (routes, group_weight[:, None], pair_weight, columns),
        flops=2 * slots * rows * rows,
    )
    expert_output = run(
        combine_kernel,
        shape((rows, width)),
        (returned, high, low),
        flops=4 * slots * rows * width,
    )
    return (mixer_output, expert_output)


def solution(mesh):
    both = ("ep", "tp")
    return jax.shard_map(
        local,
        mesh=mesh,
        in_specs=(
            P(both, None),
            P("ep", "tp"),
            P(),
            P(None, "tp"),
            P(None, "tp"),
            P(None, "tp"),
            P(None, "tp"),
            P("tp"),
            P("tp", None),
            P(both, None),
            P(),
            P(both, None),
            P(both),
            P(both, None),
            P(both, None, None),
            P(both, None, None),
            P(both, None, None),
        ),
        out_specs=(P(both, None), P(both, None)),
        check_vma=False,
    )
```

```python
import functools

import jax
import jax.numpy as jnp
import numpy as np
from jax import lax
from jax.experimental import pallas as pl
from jax.experimental.pallas import tpu as pltpu
from jax.sharding import PartitionSpec as P


KEY_DIM = 128
VALUE_DIM = 256
CHUNK = 256
CAP = 3
EPSILON = 1e-05
THETA = 10000.0
BF = jnp.bfloat16
F32 = jnp.float32
VM = pl.BlockSpec(memory_space=pltpu.VMEM)
SM = pl.BlockSpec(memory_space=pltpu.SMEM)


HBM = pl.BlockSpec(memory_space=pltpu.HBM)


def run(kernel, outs, args, scalars=0, flops=0, scratch=(), vmem=24 << 20, hbm=(), hbm_outs=()):
    nbytes = sum(a.size * a.dtype.itemsize for a in args) + sum(
        o.size * o.dtype.itemsize for o in jax.tree.leaves(outs)
    )
    return pl.pallas_call(
        kernel,
        out_shape=outs,
        in_specs=[SM if i < scalars else HBM if i in hbm else VM for i in range(len(args))],
        out_specs=tuple(HBM if i in hbm_outs else VM for i in range(len(outs)))
        if isinstance(outs, tuple)
        else VM,
        scratch_shapes=list(scratch),
        compiler_params=pltpu.CompilerParams(vmem_limit_bytes=vmem),
        cost_estimate=pl.CostEstimate(flops=flops, bytes_accessed=nbytes, transcendentals=0),
    )(*args)


def after(value, *earlier):
    return lax.optimization_barrier((value, *earlier))[0]


def shape(dims, dtype=BF):
    return jax.ShapeDtypeStruct(dims, dtype)


def dot(a, b, ca=1, cb=0):
    return lax.dot_general(a, b, (((ca,), (cb,)), ((), ())), preferred_element_type=F32)


def silu(v):
    return v * (1.0 / (1.0 + jnp.exp(-v)))


def normalised(x, gain):
    x = x.astype(F32)
    centred = x - jnp.mean(x, axis=-1, keepdims=True)
    spread = jnp.mean(centred * centred, axis=-1, keepdims=True)
    return centred * lax.rsqrt(spread + EPSILON) * gain


def begin(sems, *pairs):
    copies = [pltpu.make_async_copy(a, b, sems.at[i]) for i, (a, b) in enumerate(pairs)]
    for copy in copies:
        copy.start()
    return copies


def finish(copies):
    for copy in copies:
        copy.wait()


def fetch(sems, *pairs):
    finish(begin(sems, *pairs))


def rows_of(ref, parts):
    pairs, lower = [], 0
    for part in parts:
        pairs.append((part, ref.at[lower : lower + part.shape[0], :]))
        lower += part.shape[0]
    return pairs


def norm_kernel(x_hbm, gain_hbm, o_ref, x_ref, gain_ref, sems):
    fetch(sems, (x_hbm, x_ref), (gain_hbm, gain_ref))
    o_ref[...] = normalised(x_ref[...], gain_ref[...]).astype(BF)


def dispatch_kernel(x_hbm, gain_hbm, routes_hbm, o_ref, x_ref, gain_ref, routes_ref, sems):
    fetch(sems, (x_hbm, x_ref), (gain_hbm, gain_ref), (routes_hbm, routes_ref))
    rows = normalised(x_ref[...], gain_ref[...]).astype(BF)
    tokens = rows.shape[0]
    experts = o_ref.shape[0] * o_ref.shape[2]
    ids = lax.broadcasted_iota(jnp.int32, (experts, tokens), 0)
    named = (ids == routes_ref[0:1, :]) | (ids == routes_ref[1:2, :])
    named = jnp.where(named, 1.0, 0.0)
    before = lax.broadcasted_iota(jnp.int32, (tokens, tokens), 0) < lax.broadcasted_iota(
        jnp.int32, (tokens, tokens), 1
    )
    rank = dot(named.astype(BF), jnp.where(before, 1.0, 0.0).astype(BF))
    for slot in range(CAP):
        pick = jnp.where(rank == float(slot), named, 0.0).astype(BF)
        o_ref[:, slot] = dot(pick, rows).astype(BF).reshape(
            o_ref.shape[0], o_ref.shape[2], o_ref.shape[3]
        )


def turn_kernel(index_ref, x_ref, o_ref):
    rows = x_ref.shape[0]
    perm = lax.broadcasted_iota(jnp.int32, (rows, rows), 0) == index_ref[...]
    o_ref[...] = dot(jnp.where(perm, 1.0, 0.0).astype(BF), x_ref[...]).astype(BF)


def expert_kernel(first, x_ref, gate_ref, up_ref, down_ref, o_ref, hidden):
    step = pl.program_id(0)

    @pl.when(step < first)
    def _():
        x = x_ref[...]
        tile = gate_ref.shape[1]
        here = pl.ds(pl.multiple_of(step * tile, tile), tile)
        hidden[:, here] = (silu(dot(x, gate_ref[...])) * dot(x, up_ref[...])).astype(BF)

    @pl.when(step >= first)
    def _():
        o_ref[...] = dot(hidden[...], down_ref[...]).reshape(o_ref.shape).astype(BF)


def mix_kernel(routes_ref, group_ref, pair_ref, cols_ref, high_ref, low_ref):
    tokens = routes_ref.shape[0]
    ids = cols_ref[0:1, :]
    slots = cols_ref[1:2, :].astype(F32)
    weight = group_ref[...] * pair_ref[...]
    first = routes_ref[:, 0:1] == ids
    second = routes_ref[:, 1:2] == ids
    named = jnp.where(first | second, 1.0, 0.0).astype(BF)
    before = lax.broadcasted_iota(jnp.int32, (tokens, tokens), 1) < lax.broadcasted_iota(
        jnp.int32, (tokens, tokens), 0
    )
    rank = dot(jnp.where(before, 1.0, 0.0).astype(BF), named)
    mix = jnp.where(first, weight[:, 0:1], 0.0) + jnp.where(second, weight[:, 1:2], 0.0)
    mix = jnp.where(rank == slots, mix, 0.0)
    high = mix.astype(BF)
    high_ref[...] = high
    low_ref[...] = (mix - high.astype(F32)).astype(BF)


def combine_kernel(rows_ref, high_ref, low_ref, o_ref):
    rows = rows_ref[...].reshape(high_ref.shape[1], rows_ref.shape[2])
    o_ref[...] = (dot(high_ref[...], rows) + dot(low_ref[...], rows)).astype(BF)


def project_kernel(*refs):
    *ins, o_hbm, w_hbm, lhs, wq, wk, wv, wg, w_ref, o_ref, sems, out_sems = refs
    weights = begin(sems, *zip(ins[6:], (wq, wk, wv, wg)), *rows_of(lhs, ins[:6]))
    finish(weights[:4])
    lower = 0
    for part in (wq, wk, wv, wg):
        w_ref[:, lower : lower + part.shape[1]] = part[...]
        lower += part.shape[1]
    joined = begin(out_sems, (w_ref, w_hbm))
    finish(weights[4:])
    o_ref[...] = dot(lhs[...], w_ref[...]).astype(BF)
    fetch(sems, (o_ref, o_hbm))
    finish(joined)


def split_total(total, like):
    high = total.astype(BF).astype(F32)
    mid = (total - high).astype(BF).astype(F32)
    low = total - high - mid
    row = lax.broadcasted_iota(jnp.int32, like, 0)
    return jnp.where(row == 0, high, jnp.where(row == 1, mid, low)).astype(BF)


def prefix_sums(rows):
    n = rows.shape[1]
    upper = lax.broadcasted_iota(jnp.int32, (n, n), 0) <= lax.broadcasted_iota(jnp.int32, (n, n), 1)
    return lax.dot_general(
        rows, jnp.where(upper, 1.0, 0.0), (((1,), (0,)), ((), ())),
        precision=lax.Precision.HIGHEST, preferred_element_type=F32,
    )


AWAY = (0, 3, 1, 2)


def chunk_sums(decay_ref, steps_ref):
    steps_ref[...] = jnp.zeros(steps_ref.shape, F32)
    for i in range(decay_ref.shape[1] // CHUNK):
        steps_ref[i : i + 1, :] = decay_ref[:, i * CHUNK : (i + 1) * CHUNK]
    return prefix_sums(steps_ref[...])


def mixer_kernel(
    me_ref, early_hbm, b0, b1, b2, b3, w_hbm, cos_hbm, sin_hbm, cos0, sin0, decay,
    g_hbm, state_ref, q_hbm, k_hbm, v_hbm,
    lhs, buf, early_ref, w_ref, cos_ref, sin_ref, cos0_ref, sin0_ref, decay_ref, steps_ref,
    q_ref, k_ref, v_ref, g_ref, kept_ref, sems, late_sems,
):
    second = begin(
        late_sems,
        (decay, decay_ref),
        (early_hbm, early_ref),
        (cos_hbm, cos_ref),
        (sin_hbm, sin_ref),
        (cos0, cos0_ref),
        (sin0, sin0_ref),
    )
    first = begin(sems, (w_hbm, w_ref))
    segment, mine = me_ref[0], me_ref[1]
    y, core = mine // 2, mine % 2
    rows = 2 * b0.shape[0]
    early = early_ref.shape[0] // rows

    def placed(i, block):
        owner = (y + AWAY[i // 2]) % 4 * 2 + (core + i) % 2
        buf[pl.ds(pl.multiple_of(owner * rows, rows), rows), :] = block

    finish(second)
    sums = chunk_sums(decay_ref, steps_ref)
    columns = sums.T
    chunks = buf.shape[0] // CHUNK
    ends = [sums[i : i + 1, CHUNK - 1 : CHUNK] for i in range(chunks)]
    remain, total = [], jnp.zeros((1, 1), F32)
    for i in reversed(range(chunks)):
        remain.append(jnp.exp(total + ends[i] - columns[:, i : i + 1]))
        total = total + ends[i]
    remain = remain[::-1]
    start_cos = cos0_ref[pl.ds(segment, 1), :]
    start_sin = sin0_ref[pl.ds(segment, 1), :]
    for i in range(early):
        placed(i, early_ref[i * rows : (i + 1) * rows, :])
    for block, there in rows_of(lhs, (b0, b1, b2, b3)):
        there[...] = block[...]
    finish(first)
    late = dot(lhs[...], w_ref[...]).astype(BF)
    for i in range(2):
        placed(early + i, late[i * rows : (i + 1) * rows, :])
    v_ref[...] = buf[:, 2 * KEY_DIM : 2 * KEY_DIM + VALUE_DIM]
    g_ref[...] = buf[:, 2 * KEY_DIM + VALUE_DIM :]
    for i in range(chunks):
        here = slice(i * CHUNK, (i + 1) * CHUNK)
        cosine = cos_ref[here, :] * start_cos - sin_ref[here, :] * start_sin
        sine = sin_ref[here, :] * start_cos + cos_ref[here, :] * start_sin

        def rotated(lower):
            part = buf[here, lower : lower + KEY_DIM].astype(F32)
            return (part * cosine + pltpu.roll(part, KEY_DIM // 2, 1) * sine).astype(BF)

        key = rotated(KEY_DIM)
        k_ref[here, :] = key
        kept_ref[here, :] = (key.astype(F32) * remain[i]).astype(BF)
        q_ref[here, :] = rotated(0)
    copies = begin(late_sems, (q_ref, q_hbm), (k_ref, k_hbm), (v_ref, v_hbm), (g_ref, g_hbm))
    state_ref[0:KEY_DIM, :] = dot(kept_ref[...], v_ref[...], 0, 0).astype(BF)
    state_ref[KEY_DIM:, :] = split_total(total, (8, VALUE_DIM))
    finish(copies)


def retain_kernel(
    q_hbm, k_hbm, v_hbm, decay, local_ref, scaled_ref,
    q_ref, k_ref, v_ref, decay_ref, steps_ref, sems,
):
    copies = begin(sems, (decay, decay_ref), (q_hbm, q_ref), (k_hbm, k_ref), (v_hbm, v_ref))
    causal = lax.broadcasted_iota(jnp.int32, (CHUNK, CHUNK), 0) >= lax.broadcasted_iota(
        jnp.int32, (CHUNK, CHUNK), 1
    )
    finish(copies)
    sums = chunk_sums(decay_ref, steps_ref)
    columns = sums.T
    state, base = None, jnp.zeros((1, 1), F32)
    chunks = q_ref.shape[0] // CHUNK
    for i in range(chunks):
        here = slice(i * CHUNK, (i + 1) * CHUNK)
        query, key, value = q_ref[here, :], k_ref[here, :], v_ref[here, :]
        row, col = sums[i : i + 1, :], columns[:, i : i + 1]
        weight = jnp.where(causal, jnp.exp(jnp.minimum(col - row, 0.0)), 0.0)
        decayed = (dot(query, key, 1, 1) * weight).astype(BF)
        out = dot(decayed, value)
        wide = query.astype(F32)
        if state is not None:
            out = out + dot((wide * jnp.exp(col)).astype(BF), state.astype(BF))
        local_ref[here, :] = out
        scaled_ref[here, :] = (wide * jnp.exp(col + base)).astype(BF)
        end = row[:, CHUNK - 1 : CHUNK]
        if i < chunks - 1:
            kept = (key.astype(F32) * jnp.exp(end - col)).astype(BF)
            update = dot(kept, value, 0, 0)
            state = update if state is None else state * jnp.exp(end) + update
        base = base + end


def read_payload(ref):
    tail = ref[KEY_DIM:, :].astype(F32)
    return ref[0:KEY_DIM, :].astype(F32), tail[0:1] + tail[1:2] + tail[2:3]


def before_me(pos, parts):
    state, gone = 0.0, 0.0
    for j, (own, total) in enumerate(parts):
        between = 0.0
        for i, (_, other) in enumerate(parts):
            if i != j:
                inside = (pos[i] > pos[j]) & (pos[i] < pos[0])
                between = between + jnp.where(inside, other, 0.0)
        earlier = pos[j] < pos[0]
        state = state + jnp.where(earlier, own * jnp.exp(between), 0.0)
        gone = gone + jnp.where(earlier, total, 0.0)
    return state, gone


NEAR = (0, 3, 1, 2)


def x_kernel(me_ref, p0, p1, p2, p3, prefix_ref, gone_ref, state_ref):
    pos = [(me_ref[0] + k) % 4 for k in NEAR]
    parts = [read_payload(p) for p in (p0, p1, p2, p3)]
    state, gone = before_me(pos, parts)
    prefix_ref[...] = state
    gone_ref[...] = jnp.broadcast_to(jnp.exp(gone), gone_ref.shape)
    whole, total = 0.0, 0.0
    for j, (own, mine) in enumerate(parts):
        later = 0.0
        for i, (_, other) in enumerate(parts):
            if i != j:
                later = later + jnp.where(pos[i] > pos[j], other, 0.0)
        whole = whole + own * jnp.exp(later)
        total = total + mine
    state_ref[0:KEY_DIM, :] = whole.astype(BF)
    state_ref[KEY_DIM:, :] = split_total(total, (8, VALUE_DIM))


def gated_kernel(
    me_ref, p0, p1, p2, p3, prefix_ref, gone_ref, local_ref, scaled_ref, gate_ref,
    gain_ref, own_ref, twin_ref, buf,
):
    pos = [(me_ref[0] // 4 + k) % 4 for k in NEAR]
    parts = [read_payload(p) for p in (p0, p1, p2, p3)]
    state, _ = before_me(pos, parts)
    incoming = (prefix_ref[...] + gone_ref[0:1, :] * state).astype(BF)
    retained = local_ref[...] + dot(scaled_ref[...], incoming)
    heads = normalised(retained, gain_ref[...])
    buf[...] = (silu(gate_ref[...].astype(F32)) * heads).astype(BF)
    core = me_ref[1] % 2
    rows = own_ref.shape[0] // 4
    for y in range(4):
        there = slice(y * rows, (y + 1) * rows)
        own_ref[there, :] = buf[pl.ds(pl.multiple_of((2 * y + core) * rows, rows), rows), :]
        twin_ref[there, :] = buf[pl.ds(pl.multiple_of((2 * y + 1 - core) * rows, rows), rows), :]


def output_kernel(me_ref, own_ref, twin_ref, wo_ref, wt_ref, o0, o1, o2, o3, lhs, lht):
    rows = o0.shape[0]
    for k in range(4):
        here = slice(k * rows, (k + 1) * rows)
        y = (me_ref[1] // 2 + (0, 1, 3, 2)[k]) % 4
        there = pl.ds(pl.multiple_of(y * rows, rows), rows)
        lhs[here, :] = own_ref[there, :]
        lht[here, :] = twin_ref[there, :]
    out = (dot(lhs[...], wo_ref[...]) + dot(lht[...], wt_ref[...])).astype(BF)
    for k, ref in enumerate((o0, o1, o2, o3)):
        ref[...] = out[k * rows : (k + 1) * rows, :]


def sum_kernel(a, b, c, d, o_ref):
    o_ref[...] = (
        a[...].astype(F32) + b[...].astype(F32) + c[...].astype(F32) + d[...].astype(F32)
    ).astype(BF)


def core_swap(x):
    return lax.ppermute(x, "tp", [(t, t ^ 1) for t in range(8)])


def y_shift(x, k):
    return lax.ppermute(x, "tp", [(t, ((t // 2 + k) % 4) * 2 + t % 2) for t in range(8)])


def x_shift(x, k):
    return lax.ppermute(x, "ep", [(e, (e // 4) * 4 + (e + k) % 4) for e in range(16)])


def z_shift(x, k):
    return lax.ppermute(x, "ep", [(e, (e + 4 * k) % 16) for e in range(16)])


def exchange(x, axis):
    return lax.all_to_all(x, axis, split_axis=0, concat_axis=0, tiled=True)


def rotation(positions):
    half = KEY_DIM // 2
    frequency = THETA ** (-np.arange(half) / half)
    angles = positions[:, None].astype(np.float64) * frequency[None, :]
    cosine, sine = np.cos(angles), np.sin(angles)
    return (
        np.concatenate([cosine, cosine], axis=1).astype(np.float32),
        np.concatenate([-sine, sine], axis=1).astype(np.float32),
    )


def local(
    mixer_input,
    log_decay,
    mixer_gain,
    query_weight,
    key_weight,
    value_weight,
    gate_weight,
    head_gain,
    output_weight,
    expert_input,
    expert_gain,
    routes,
    group_weight,
    pair_weight,
    expert_gate,
    expert_up,
    expert_down,
):
    rows, width = mixer_input.shape
    seg_rows = log_decay.shape[0]
    ep, tp = lax.axis_index("ep"), lax.axis_index("tp")
    n_ep, n_tp = lax.axis_size("ep"), lax.axis_size("tp")
    slots = n_ep * n_tp * CAP
    me = jnp.stack([ep, tp]).astype(jnp.int32)

    sems = lambda n: pltpu.SemaphoreType.DMA((n,))
    normed = run(
        norm_kernel,
        shape((rows, width)),
        (mixer_input, mixer_gain[None]),
        hbm=(0, 1),
        vmem=60 << 20,
        scratch=(pltpu.VMEM((rows, width), BF), pltpu.VMEM((1, width), F32), sems(2)),
    )
    from_below = y_shift(normed, 1)
    from_above = y_shift(normed, -1)
    twin = core_swap(normed)

    outgoing = run(
        dispatch_kernel,
        shape((n_ep, CAP, n_tp, width)),
        (after(expert_input, normed, me), expert_gain[None], routes.T),
        flops=2 * slots * rows * width,
        hbm=(0, 1, 2),
        vmem=60 << 20,
        scratch=(
            pltpu.VMEM((rows, width), BF),
            pltpu.VMEM((1, width), F32),
            pltpu.VMEM((2, rows), jnp.int32),
            sems(3),
        ),
    )
    staged = exchange(outgoing, "ep")

    twin_out = core_swap(output_weight)
    weights = (query_weight, key_weight, value_weight, gate_weight)
    cols = sum(w.shape[1] for w in weights)
    cosine, sine = rotation(np.arange(seg_rows))
    cosine_start, sine_start = rotation(np.arange(n_ep) * seg_rows)
    half = rows // 2
    far_low = y_shift(from_below[:half], 1)
    far_high = y_shift(from_above[half:], -1)
    below_twin, above_twin = core_swap(from_below), core_swap(from_above)
    early, joined = run(
        project_kernel,
        (shape((6 * rows, cols)), shape((width, cols))),
        (
            normed,
            twin, from_below, below_twin, from_above, above_twin,
            *weights,
        ),
        flops=2 * 6 * rows * width * cols,
        hbm=range(10),
        hbm_outs=(0, 1),
        vmem=60 << 20,
        scratch=(
            pltpu.VMEM((6 * rows, width), BF),
            *(pltpu.VMEM(w.shape, BF) for w in weights),
            pltpu.VMEM((width, cols), BF),
            pltpu.VMEM((6 * rows, cols), BF),
            sems(10),
            sems(1),
        ),
    )
    low_twin, high_twin = core_swap(far_low), core_swap(far_high)
    gate, state, query, key, value = run(
        mixer_kernel,
        (
            shape((seg_rows, VALUE_DIM)),
            shape((KEY_DIM + 8, VALUE_DIM)),
            shape((seg_rows, KEY_DIM)),
            shape((seg_rows, KEY_DIM)),
            shape((seg_rows, VALUE_DIM)),
        ),
        (
            me, early, far_low, far_high, low_twin, high_twin, joined,
            cosine, sine, cosine_start, sine_start, log_decay.T,
        ),
        scalars=1,
        flops=2 * 2 * rows * width * cols,
        hbm=(1, 6, 7, 8, 9, 10, 11),
        hbm_outs=(0, 2, 3, 4),
        vmem=60 << 20,
        scratch=(
            pltpu.VMEM((2 * rows, width), BF),
            pltpu.VMEM((seg_rows, cols), BF),
            pltpu.VMEM((6 * rows, cols), BF),
            pltpu.VMEM((width, cols), BF),
            pltpu.VMEM((seg_rows, KEY_DIM), F32),
            pltpu.VMEM((seg_rows, KEY_DIM), F32),
            pltpu.VMEM((n_ep, KEY_DIM), F32),
            pltpu.VMEM((n_ep, KEY_DIM), F32),
            pltpu.VMEM((1, seg_rows), F32),
            pltpu.VMEM((8, CHUNK), F32),
            pltpu.VMEM((seg_rows, KEY_DIM), BF),
            pltpu.VMEM((seg_rows, KEY_DIM), BF),
            pltpu.VMEM((seg_rows, VALUE_DIM), BF),
            pltpu.VMEM((seg_rows, VALUE_DIM), BF),
            pltpu.VMEM((seg_rows, KEY_DIM), BF),
            sems(5),
            sems(6),
        ),
    )

    index = jnp.arange(slots, dtype=jnp.int32)
    deep = n_ep * CAP
    to_tp = ((index % n_tp) * deep + index // n_tp)[None]
    turned = run(
        turn_kernel,
        shape((slots, width)),
        (to_tp, after(staged, state).reshape(slots, width)),
        flops=2 * slots * slots * width,
    )
    tokens = exchange(turned.reshape(n_tp, deep, width), "tp").reshape(slots, width)

    payloads = (state, x_shift(state, 1), x_shift(state, -1), x_shift(state, 2))
    prefix, gone, plane = run(
        x_kernel,
        (
            shape((KEY_DIM, VALUE_DIM), F32),
            shape((8, VALUE_DIM), F32),
            shape((KEY_DIM + 8, VALUE_DIM)),
        ),
        (me, *payloads),
        scalars=1,
    )
    planes = (plane, z_shift(plane, 1), z_shift(plane, -1), z_shift(plane, 2))
    local_out, scaled = run(
        retain_kernel,
        (shape((seg_rows, VALUE_DIM), F32), shape((seg_rows, KEY_DIM))),
        (query, key, value, log_decay.T),
        flops=8 * seg_rows * CHUNK * VALUE_DIM,
        hbm=range(4),
        scratch=(
            pltpu.VMEM((seg_rows, KEY_DIM), BF),
            pltpu.VMEM((seg_rows, KEY_DIM), BF),
            pltpu.VMEM((seg_rows, VALUE_DIM), BF),
            pltpu.VMEM((1, seg_rows), F32),
            pltpu.VMEM((8, CHUNK), F32),
            sems(4),
        ),
    )
    own_gated, twin_gated = run(
        gated_kernel,
        (shape((4 * rows, VALUE_DIM)), shape((4 * rows, VALUE_DIM))),
        (me, *planes, prefix, gone, local_out, scaled, gate, head_gain[None]),
        scalars=1,
        flops=2 * seg_rows * KEY_DIM * VALUE_DIM,
        scratch=(pltpu.VMEM((seg_rows, VALUE_DIM), BF),),
    )
    inner = expert_gate.shape[2]
    tile, wide = 512, 1024
    first = inner // tile
    experts = pl.pallas_call(
        functools.partial(expert_kernel, first),
        grid=(first + width // wide,),
        out_shape=shape((n_ep * n_tp, CAP, width)),
        in_specs=[
            pl.BlockSpec((slots, width), lambda f: (0, 0)),
            pl.BlockSpec((width, tile), lambda f: (0, jnp.minimum(f, first - 1))),
            pl.BlockSpec((width, tile), lambda f: (0, jnp.minimum(f, first - 1))),
            pl.BlockSpec((inner, wide), lambda f: (0, jnp.maximum(f - first, 0))),
        ],
        out_specs=pl.BlockSpec(
            (n_ep * n_tp, CAP, wide), lambda f: (0, 0, jnp.maximum(f - first, 0))
        ),
        scratch_shapes=[pltpu.VMEM((slots, inner), BF)],
        compiler_params=pltpu.CompilerParams(
            vmem_limit_bytes=60 << 20, dimension_semantics=("arbitrary",)
        ),
        cost_estimate=pl.CostEstimate(
            flops=6 * slots * width * inner, bytes_accessed=6 * width * inner, transcendentals=0
        ),
    )
    other_gated = core_swap(twin_gated)
    kept, up, down, far = run(
        output_kernel,
        tuple(shape((rows, width)) for _ in range(4)),
        (me, own_gated, other_gated, output_weight, twin_out),
        scalars=1,
        flops=2 * 4 * rows * 2 * VALUE_DIM * width,
        scratch=(pltpu.VMEM((4 * rows, VALUE_DIM), BF), pltpu.VMEM((4 * rows, VALUE_DIM), BF)),
    )
    got_far = y_shift(far, 2)
    got_up = y_shift(up, 1)
    got_down = y_shift(down, -1)
    results = experts(after(tokens, kept), expert_gate[0], expert_up[0], expert_down[0])
    mixer_output = run(sum_kernel, shape((rows, width)), (kept, got_up, got_down, got_far))

    returned = exchange(results, ("tp", "ep"))
    columns = jnp.stack([index % deep // CAP * n_tp + index // deep, index % CAP])
    high, low = run(
        mix_kernel,
        (shape((rows, slots)), shape((rows, slots))),
        (routes, group_weight[:, None], pair_weight, columns),
        flops=2 * slots * rows * rows,
    )
    expert_output = run(
        combine_kernel,
        shape((rows, width)),
        (returned, high, low),
        flops=4 * slots * rows * width,
    )
    return (mixer_output, expert_output)


def solution(mesh):
    both = ("ep", "tp")
    return jax.shard_map(
        local,
        mesh=mesh,
        in_specs=(
            P(both, None),
            P("ep", "tp"),
            P(),
            P(None, "tp"),
            P(None, "tp"),
            P(None, "tp"),
            P(None, "tp"),
            P("tp"),
            P("tp", None),
            P(both, None),
            P(),
            P(both, None),
            P(both),
            P(both, None),
            P(both, None, None),
            P(both, None, None),
            P(both, None, None),
        ),
        out_specs=(P(both, None), P(both, None)),
        check_vma=False,
    )
```
